32 devices in a mesh: fs: 8 (over z, y), tp: 4 (over x, core).
Axes of the slice: x: 2, y: 2, z: 4, core: 2. Of those that a mesh axis runs over, the one named last changes fastest.
Arguments:
- tokens: bfloat16 [2048, 2048], P('fs', 'tp'), may hold values from -12.1 to 12.1, as said below
- gate_weight: float32 [2048, 5632], P('fs', 'tp'), may hold values from -0.125 to 0.125
- up_weight: float32 [2048, 5632], P('fs', 'tp'), may hold values from -0.125 to 0.125
- down_weight: float32 [5632, 2048], P('tp', 'fs'), may hold values from -0.078125 to 0.078125
- gate_scale: float32 [4, 1408], P('tp', 'fs'), may hold values from 0.1 to 1.9
- up_scale: float32 [4, 1408], P('tp', 'fs'), may hold values from 0.1 to 1.9
- down_scale: float32 [4, 512], P('tp', 'fs'), may hold values from 0.16 to 4.6, as said below
- bgate_weight: float32 [2048, 2048], P('fs', 'tp'), may hold values from -0.125 to 0.125
- cgate_weight: float32 [2048, 2048], P('fs', 'tp'), may hold values from -0.125 to 0.125
- value_weight: float32 [2048, 2048], P('fs', 'tp'), may hold values from -0.125 to 0.125
- bgate_scale: float32 [4, 512], P('tp', 'fs'), may hold values from 0.1 to 1.9
- cgate_scale: float32 [4, 512], P('tp', 'fs'), may hold values from 0.1 to 1.9
- value_scale: float32 [4, 512], P('tp', 'fs'), may hold values from 0.1 to 1.9
- conv_taps: float32 [3, 2048], replicated, may hold values from -3.5 to 3.5
- mixout_weight: float32 [2048, 2048], P('tp', 'fs'), may hold values from -0.125 to 0.125
- mixout_scale: float32 [4, 512], P('tp', 'fs'), may hold values from 0.16 to 4.6, as said below
- first_gain: float32 [2048], replicated, may hold values from 0.1 to 1.9
- first_shift: float32 [2048], replicated, may hold values from -1.8 to 1.8
- mixer_gain: float32 [2048], replicated, may hold values from 0.1 to 1.9
- mixer_shift: float32 [2048], replicated, may hold values from -1.8 to 1.8
- last_gain: float32 [2048], replicated, may hold values from 0.1 to 1.9
- last_shift: float32 [2048], replicated, may hold values from -1.8 to 1.8
Outputs:
- layer_out: bfloat16 [2048, 2048], P('fs', 'tp')
The draws below stay inside these ranges and needn't reach their ends.
Inputs may be any that keep to these rules, and one draw needn't show every extreme that they name: `tokens`: normal values times one factor for each of 4 equal consecutive blocks of the features. `down_scale`: positive; one factor for each row times a spread over the columns. `mixout_scale`: positive; one factor for each row times a spread over the columns.
All inputs are finite; a program needn't handle non-finite values.
Results may differ from the reference program's by a relative error of at most 0.025.
Values may be sent and summed in bfloat16 or wider, within the bound.
A program may use at most 64 MiB of HBM per device.

```python
import jax
import jax.numpy as jnp
from jax import lax

D = 2048
FF = 5632
CONV_CH = 2048
TAPS = 3
LENGTH = 128
TOKENS = 2048
N_TP = 4


def block_factors(key, blocks):
    return jnp.exp(jax.random.uniform(key, (blocks, 1), jnp.float32, -1.1, 1.1))


def draw_tokens(key, part):
    values = jnp.clip(jax.random.normal(jax.random.fold_in(key, 11), (TOKENS, D), jnp.float32), -4.0, 4.0)
    factor = block_factors(jax.random.fold_in(key, 12), N_TP)
    column_factor = jnp.repeat(factor[:, 0], D // N_TP)
    return (values * column_factor[None, :]).astype(jnp.bfloat16)


def column_scale(key):
    factor = block_factors(jax.random.fold_in(key, 1), N_TP)
    spread_part = jax.random.uniform(jax.random.fold_in(key, 2), (N_TP, D // N_TP), jnp.float32, 0.7, 1.3)
    return factor * spread_part


def draw_down_scale(key, part):
    return column_scale(jax.random.fold_in(key, 21))


def draw_mixout_scale(key, part):
    return column_scale(jax.random.fold_in(key, 22))


def block_levels(stream_key, dims, split, smallest, high):
    factor_of, own = 1.0, jax.random.fold_in(stream_key, 6)
    for axis_at, blocks in split:
        draws = jnp.exp(jax.random.uniform(jax.random.fold_in(own, axis_at), (blocks,), jnp.float32, smallest / len(split), high / len(split)))
        factor_of = factor_of * jnp.repeat(draws, dims[axis_at] // blocks).reshape([-1 if axis == axis_at else 1 for axis in range(len(dims))])
    return factor_of


def scatter_about(key, shape, scale, bound, cuts=(), held_as=jnp.bfloat16):
    values = scale * jax.random.normal(key, shape, jnp.float32)
    if cuts:
        values = values * block_levels(key, shape, cuts, -0.22, 0.18)
    return jnp.clip(values, -bound, bound).astype(held_as)


def setup_inputs(seed: int = 0) -> dict:
    key_list = jax.random.split(jax.random.key(seed), 23)
    return {
        "tokens": draw_tokens(jax.random.fold_in(key_list[22], 71), 0),
        "gate_weight": scatter_about(key_list[1], (D, FF), D ** -0.5, 0.125, ((0, 8), (1, 4)), jnp.float32),
        "up_weight": scatter_about(key_list[2], (D, FF), D ** -0.5, 0.125, ((0, 8), (1, 4)), jnp.float32),
        "down_weight": scatter_about(key_list[3], (FF, D), FF ** -0.5, 0.078125, ((0, 4), (1, 8)), jnp.float32),
        "gate_scale": jnp.clip(1.0 + 0.18 * jax.random.normal(key_list[4], (N_TP, FF // N_TP), jnp.float32), 0.1, 1.9),
        "up_scale": jnp.clip(1.0 + 0.18 * jax.random.normal(key_list[5], (N_TP, FF // N_TP), jnp.float32), 0.1, 1.9),
        "down_scale": draw_down_scale(jax.random.fold_in(key_list[22], 71), 0),
        "bgate_weight": scatter_about(key_list[7], (D, CONV_CH), D ** -0.5, 0.125, ((0, 8), (1, 4)), jnp.float32),
        "cgate_weight": scatter_about(key_list[8], (D, CONV_CH), D ** -0.5, 0.125, ((0, 8), (1, 4)), jnp.float32),
        "value_weight": scatter_about(key_list[9], (D, CONV_CH), D ** -0.5, 0.125, ((0, 8), (1, 4)), jnp.float32),
        "bgate_scale": jnp.clip(1.0 + 0.18 * jax.random.normal(key_list[10], (N_TP, CONV_CH // N_TP), jnp.float32), 0.1, 1.9),
        "cgate_scale": jnp.clip(1.0 + 0.18 * jax.random.normal(key_list[11], (N_TP, CONV_CH // N_TP), jnp.float32), 0.1, 1.9),
        "value_scale": jnp.clip(1.0 + 0.18 * jax.random.normal(key_list[12], (N_TP, CONV_CH // N_TP), jnp.float32), 0.1, 1.9),
        "conv_taps": scatter_about(key_list[13], (TAPS, CONV_CH), TAPS ** -0.5, 3.5, (), jnp.float32),
        "mixout_weight": scatter_about(key_list[14], (CONV_CH, D), CONV_CH ** -0.5, 0.125, ((0, 4), (1, 8)), jnp.float32),
        "mixout_scale": draw_mixout_scale(jax.random.fold_in(key_list[22], 71), 0),
        "first_gain": jnp.clip(1.0 + 0.18 * jax.random.normal(key_list[16], (D,), jnp.float32), 0.1, 1.9),
        "first_shift": scatter_about(key_list[17], (D,), 0.3, 1.8, (), jnp.float32),
        "mixer_gain": jnp.clip(1.0 + 0.18 * jax.random.normal(key_list[18], (D,), jnp.float32), 0.1, 1.9),
        "mixer_shift": scatter_about(key_list[19], (D,), 0.3, 1.8, (), jnp.float32),
        "last_gain": jnp.clip(1.0 + 0.18 * jax.random.normal(key_list[20], (D,), jnp.float32), 0.1, 1.9),
        "last_shift": scatter_about(key_list[21], (D,), 0.3, 1.8, (), jnp.float32),
    }


RESIDUAL_SCALE = 1.4142135623730951
HALF_STEP = 0.5
EPSILON = 1e-05

def post_norm(residual, branch, norm_gain, norm_shift):
    summed = RESIDUAL_SCALE * residual.astype(jnp.float32) + branch
    average = lax.optimization_barrier(jnp.mean(summed, -1, keepdims=True))
    mean_square = lax.optimization_barrier(jnp.mean(summed * summed, -1, keepdims=True))
    variance = mean_square - average * average
    return ((summed - average) * lax.rsqrt(variance + EPSILON) * norm_gain + norm_shift).astype(jnp.bfloat16)

def block_sum(left_rows, right_cols):
    block_width = left_rows.shape[1] // N_TP
    running = jnp.zeros((left_rows.shape[0], right_cols.shape[1]), jnp.float32)
    for block_index in range(N_TP):
        low = block_index * block_width
        partial_value = jnp.dot(left_rows[:, low:low + block_width], right_cols[low:low + block_width], preferred_element_type=jnp.float32)
        running = running + lax.optimization_barrier(partial_value.astype(jnp.bfloat16)).astype(jnp.float32)
    return running

def scaled_dot(inputs, matrix, scales):
    product = jnp.dot(inputs, matrix.astype(jnp.bfloat16), preferred_element_type=jnp.float32)
    return product * scales.reshape(-1)

def feed(inputs, gate_weight, up_weight, down_weight, gate_scale, up_scale, down_scale):
    gate_sum = scaled_dot(inputs, gate_weight, gate_scale)
    up_sum = scaled_dot(inputs, up_weight, up_scale)
    hidden = (jax.nn.silu(gate_sum) * up_sum).astype(jnp.bfloat16)
    result = block_sum(hidden, down_weight.astype(jnp.bfloat16)) * down_scale.reshape(-1)
    return HALF_STEP * result

def causal_conv(mixed, conv_taps):
    channels = mixed.shape[1]
    shaped = mixed.reshape(-1, LENGTH, channels)
    padded = jnp.pad(shaped, ((0, 0), (TAPS - 1, 0), (0, 0)))
    convolved = jnp.zeros(shaped.shape, jnp.float32)
    for tap_index in range(TAPS):
        convolved = convolved + conv_taps[tap_index] * padded[:, tap_index:tap_index + LENGTH]
    return convolved.reshape(-1, channels)

def reference(tokens, gate_weight, up_weight, down_weight, gate_scale, up_scale, down_scale, bgate_weight, cgate_weight, value_weight, bgate_scale, cgate_scale, value_scale, conv_taps, mixout_weight, mixout_scale, first_gain, first_shift, mixer_gain, mixer_shift, last_gain, last_shift):
    ffn_args = (gate_weight, up_weight, down_weight, gate_scale, up_scale, down_scale)
    first = post_norm(tokens, feed(tokens, *ffn_args), first_gain, first_shift)
    outgate = scaled_dot(first, bgate_weight, bgate_scale)
    ingate = scaled_dot(first, cgate_weight, cgate_scale)
    values = scaled_dot(first, value_weight, value_scale)
    convolved = causal_conv(ingate * values, conv_taps)
    gated = (outgate * convolved).astype(jnp.bfloat16)
    token_mix = block_sum(gated, mixout_weight.astype(jnp.bfloat16)) * mixout_scale.reshape(-1)
    second = post_norm(first, token_mix, mixer_gain, mixer_shift)
    return post_norm(second, feed(second, *ffn_args), last_gain, last_shift)
```

```python
import functools

import jax
import jax.numpy as jnp
from jax import lax
from jax.experimental import pallas as pl
from jax.experimental.pallas import tpu as pltpu
from jax.sharding import Mesh
from jax.sharding import PartitionSpec as P

TAPS = 3
LENGTH = 128
CORES = 2

RESIDUAL_SCALE = 1.4142135623730951
HALF_STEP = 0.5
EPSILON = 1e-05
BY_AXIS = pl.DeviceIdType.MESH
ANY = pl.BlockSpec(memory_space=pl.ANY)
VMEM = pl.BlockSpec(memory_space=pltpu.VMEM)


def greet(depth, axes, others=()):
    barrier = pltpu.get_barrier_semaphore()
    z = lax.axis_index("z")
    targets = [{"z": lax.rem(z + d, depth)} for d in range(1, depth)]
    targets += [{axis: 1 - lax.axis_index(axis)} for axis in axes]
    targets += others
    for target in targets:
        pl.semaphore_signal(barrier, inc=1, device_id=target, device_id_type=BY_AXIS)
    pl.semaphore_wait(barrier, len(targets))


def remote(src, dst, send, recv, target):
    return pltpu.make_async_remote_copy(
        src_ref=src, dst_ref=dst, send_sem=send, recv_sem=recv, device_id=target, device_id_type=BY_AXIS
    )


def line_partners(z):
    near = z + 1 - 2 * lax.rem(z, 2)
    return near, lax.rem(z + 2, 4), 3 - z, lax.rem((z + 1) // 2, 2)


def line_sends(z, own, slot, send, recv):
    near, cross, opposite, middle = line_partners(z)

    @pl.when(middle == 0)
    def _():
        remote(own, slot(2), send.at[0], recv.at[2], {"z": cross}).start()

    @pl.when(middle == 1)
    def _():
        remote(own, slot(3), send.at[0], recv.at[3], {"z": opposite}).start()

    remote(own, slot(1), send.at[1], recv.at[1], {"z": near}).start()


def line_waits(z, own, slot, send, recv):
    near, cross, opposite, middle = line_partners(z)
    for k in range(2):
        remote(own, slot(1), send.at[k], recv.at[1], {"z": near}).wait_send()

    @pl.when(middle == 1)
    def _():
        for e in (2, 3):
            remote(slot(e), slot(5 - e), send.at[e + 2], recv.at[5 - e], {"z": near}).wait_send()


def block_place(ref, px, pz, py, width):
    start = pl.multiple_of((pz * 2 + py) * width, width)
    return ref.at[:, px, :, pl.ds(start, width)]


def weights_kernel(
    depth, w_ref, m_ref, s_ref, t_ref, g_ref, held_ref, sa_ref, ta_ref,
    zsend, zrecv, ysend, yrecv, xsend, xrecv, dsend, drecv, msend, mrecv,
    ssend, srecv, tzsend, tzrecv, tcsend, tcrecv, local,
):
    z, y, x, c = (lax.axis_index(axis) for axis in ("z", "y", "x", "c"))
    width = w_ref.shape[-1]
    greet(depth, ("y", "x", "c"))

    mats = w_ref.shape[1]

    def place(px, pz, py, piece=slice(None)):
        start = pl.multiple_of((pz * 2 + py) * width, width)
        return g_ref.at[piece, px, :, pl.ds(start, width)]

    to_x, to_y, to_c = {"x": 1 - x}, {"y": 1 - y}, {"c": 1 - c}
    scale_sends, z_copies, m_copies = [], [], []
    keeps = [
        pltpu.make_async_copy(s_ref, sa_ref.at[c, x, y, z], local.at[0]),
        pltpu.make_async_copy(t_ref, ta_ref.at[0, c], local.at[1]),
        pltpu.make_async_copy(w_ref.at[z], place(x, z, y), local.at[2]),
        pltpu.make_async_copy(m_ref.at[z], held_ref.at[0], local.at[3]),
    ]
    for copy in keeps:
        copy.start()
    beside = [remote(t_ref, ta_ref.at[0, c], tcsend.at[0], tcrecv.at[0], to_c)]
    beside[0].start()
    y_copies, x_copies, d_copies = [], [], []
    for p in range(mats):
        y_copies.append(remote(w_ref.at[z, p], place(x, z, y, p), ysend.at[p], yrecv.at[p], to_y))
        x_copies.append(remote(w_ref.at[z, p], place(x, z, y, p), xsend.at[p], xrecv.at[p], to_x))
        y_copies[p].start()
        x_copies[p].start()
    for d in range(1, depth):
        target = {"z": lax.rem(z + d, depth)}
        scale_sends.append(remote(s_ref, sa_ref.at[c, x, y, z], ssend.at[d], srecv.at[d], target))
        scale_sends[-1].start()
    for d in range(1, depth):
        target = lax.rem(z + d, depth)
        for p in range(mats):
            slot = d * mats + p
            z_copies.append(
                remote(w_ref.at[target, p], place(x, z, y, p), zsend.at[slot], zrecv.at[slot], {"z": target})
            )
            z_copies[-1].start()
    near, cross, opposite, middle = line_partners(z)
    line_sends(z, t_ref, lambda e: ta_ref.at[e, c], tzsend, tzrecv)
    for d in range(1, depth):
        target = lax.rem(z + d, depth)
        m_copies.append(remote(m_ref.at[target], held_ref.at[d], msend.at[d], mrecv.at[d], {"z": target}))
        m_copies[-1].start()

    def relay(e):
        d, p = divmod(e, mats)
        source = lax.rem(z - d + depth, depth)
        if e % 2 == 0:
            y_copies[e].wait_recv()
            block = place(x, source, 1 - y, p)
            copy = remote(block, block, dsend.at[e], drecv.at[e], to_x)
        else:
            x_copies[e].wait_recv()
            block = place(1 - x, source, y, p)
            copy = remote(block, block, dsend.at[e], drecv.at[e], to_y)
        copy.start()
        d_copies.append(copy)

    keeps[0].wait()
    for copy in scale_sends:
        copy.wait()
    hops = (sa_ref.at[c, x, y], sa_ref.at[c, x], sa_ref.at[c])
    for k, (part, target) in enumerate(zip(hops, (to_y, to_x, to_c))):
        slot = (0, depth, depth + 1)[k]
        hop = remote(part, part, ssend.at[slot], srecv.at[slot], target)
        hop.start()
        hop.wait()
    count = depth * mats
    for e in range(mats, count):
        d, p = divmod(e, mats)
        block = place(x, lax.rem(z - d + depth, depth), y, p)
        z_copies[e - mats].wait_recv()
        ycopy = remote(block, block, ysend.at[e], yrecv.at[e], to_y)
        xcopy = remote(block, block, xsend.at[e], xrecv.at[e], to_x)
        ycopy.start()
        xcopy.start()
        y_copies.append(ycopy)
        x_copies.append(xcopy)
        relay(e - mats)
    for e in range(count - mats, count):
        relay(e)
    for e in (1, 3, 2):
        piece = ta_ref.at[e, c]
        remote(piece, piece, tzsend.at[e], tzrecv.at[e], {"z": near}).wait_recv()
        if e > 1:
            @pl.when(middle == 1)
            def _():
                remote(piece, ta_ref.at[5 - e, c], tzsend.at[e + 2], tzrecv.at[5 - e], {"z": near}).start()
        copy = remote(piece, piece, tcsend.at[e], tcrecv.at[e], to_c)
        copy.start()
        beside.append(copy)
    for e in range(count):
        (x_copies if e % 2 == 0 else y_copies)[e].wait_recv()
        d_copies[e].wait()
        y_copies[e].wait_send()
        x_copies[e].wait_send()
    for copy in beside:
        copy.wait()
    for copy in m_copies:
        copy.wait()
    for copy in z_copies:
        copy.wait_send()
    line_waits(z, t_ref, lambda e: ta_ref.at[e, c], tzsend, tzrecv)
    for copy in keeps[1:]:
        copy.wait()


def spread_weights(depth, blocks, mixer_blocks, scale_block, own_rows):
    mats, rows, width = blocks.shape[1:]
    dma = pltpu.SemaphoreType.DMA
    return pl.pallas_call(
        functools.partial(weights_kernel, depth),
        out_shape=(
            jax.ShapeDtypeStruct((mats, 2, rows, depth * 2 * width), jnp.bfloat16),
            jax.ShapeDtypeStruct(mixer_blocks.shape, jnp.bfloat16),
            jax.ShapeDtypeStruct((CORES, 2, 2, depth) + scale_block.shape, jnp.float32),
            jax.ShapeDtypeStruct((depth, CORES) + own_rows.shape, jnp.bfloat16),
        ),
        in_specs=[ANY] * 4,
        out_specs=(ANY,) * 4,
        scratch_shapes=[dma((depth * mats,)) for _ in range(8)]
        + [dma((depth,)), dma((depth,))]
        + [dma((depth + 2,)), dma((depth + 2,))]
        + [dma((depth + 2,)) for _ in range(4)]
        + [dma((4,))],
        compiler_params=pltpu.CompilerParams(collective_id=0, has_side_effects=True),
        name="spread_weights",
    )(blocks, mixer_blocks, scale_block, own_rows)


def dot_last(left, right):
    return lax.dot_general(left, right, (((1,), (1,)), ((), ())), preferred_element_type=jnp.float32)


def merged(ref, k):
    two, rows, features = ref.shape[1:]
    return ref[k].reshape(two * rows, features)


def feed_chunk(inputs, weights, factors, taps):
    gate_sum = dot_last(inputs, merged(weights, 0)) * factors[0:1]
    up_sum = dot_last(inputs, merged(weights, 1)) * factors[1:2]
    hidden = (gate_sum / (1.0 + jnp.exp(-gate_sum)) * up_sum).astype(jnp.bfloat16)
    return jnp.dot(hidden, merged(weights, 2), preferred_element_type=jnp.float32)


def mixer_chunk(inputs, weights, factors, taps):
    outgate = dot_last(inputs, merged(weights, 0)) * factors[0:1]
    ingate = dot_last(inputs, merged(weights, 1)) * factors[1:2]
    values = dot_last(inputs, merged(weights, 2)) * factors[2:3]
    mixed = ingate * values
    position = lax.rem(lax.broadcasted_iota(jnp.int32, mixed.shape, 0), LENGTH)
    convolved = taps[TAPS - 1 : TAPS] * mixed
    for back in range(1, TAPS):
        earlier = jnp.where(position >= back, pltpu.roll(mixed, back, 0), 0.0)
        convolved = convolved + taps[TAPS - 1 - back : TAPS - back] * earlier
    gated = (outgate * convolved).astype(jnp.bfloat16)
    return jnp.dot(gated, merged(weights, 3), preferred_element_type=jnp.float32)


def stage_kernel(depth, chunk, first, final, *refs):
    refs = list(refs)
    take = lambda n: [refs.pop(0) for _ in range(n)]
    w_ref, f_ref, k_ref, own_ref, scale_ref, gain_ref, shift_ref = take(7)
    if first:
        whole, held_ref = take(2)
        out_ref, m_ref = take(2)
    else:
        (out_ref,) = take(1)
    part, half, sums, got, extra, hsend, hrecv, rsend, rrecv, esend, erecv = take(11)
    z, c = lax.axis_index("z"), lax.axis_index("c")
    near, cross, opposite, middle = line_partners(z)
    to_c = {"c": 1 - c}
    if first:
        ysend, yrecv, xsend, xrecv, dsend, drecv, local = take(7)
        y, x = lax.axis_index("y"), lax.axis_index("x")
        greet(depth, ("y", "x", "c"))
        width = held_ref.shape[-1]
        y_copies, x_copies, d_copies, keeps = [], [], [], []
        for d in range(depth):
            block = block_place(m_ref, x, lax.rem(z - d + depth, depth), y, width)
            y_copies.append(remote(held_ref.at[d], block, ysend.at[d], yrecv.at[d], {"y": 1 - y}))
            x_copies.append(remote(held_ref.at[d], block, xsend.at[d], xrecv.at[d], {"x": 1 - x}))
            keeps.append(pltpu.make_async_copy(held_ref.at[d], block, local.at[d]))
            y_copies[d].start()
            x_copies[d].start()
            keeps[d].start()
    else:
        whole, zsend, zrecv, csend, crecv = take(5)
        if final:
            sheet, fsend, frecv = take(3)
            x = lax.axis_index("x")
            greet(depth, ("x", "c"), [{"x": 1 - x, "c": 1 - c}])
        else:
            greet(depth, ("c",))
        beside = remote(own_ref, whole.at[0, c], csend.at[0], crecv.at[0], to_c)
        beside.start()
        line_sends(z, own_ref, lambda e: whole.at[e, c], zsend, zrecv)
        whole[0, c] = own_ref[...]

    def to_near(d):
        return remote(sums.at[d], got.at[1], rsend.at[d], rrecv.at[1], {"z": near})

    def to_merge(d):
        return remote(sums.at[d], extra.at[5 - d], rsend.at[d], erecv.at[5 - d], {"z": near})

    def to_cross():
        return remote(sums.at[2], got.at[2], rsend.at[2], rrecv.at[2], {"z": cross})

    def to_opposite():
        return remote(sums.at[3], got.at[3], rsend.at[3], rrecv.at[3], {"z": opposite})

    def handover(d):
        return remote(part.at[d, 1 - c], half.at[d], hsend.at[d], hrecv.at[d], to_c)

    def forward(d):
        return remote(whole.at[d, c], whole.at[d, c], csend.at[d], crecv.at[d], to_c)

    def step(i, carry):
        if first:
            d = (1 - middle) * (3 - i) + middle * lax.rem(i + 1, depth)
        else:
            d = i + middle * (i // 2) * (5 - 2 * i)

            @pl.when(d > 0)
            def _():
                remote(own_ref, whole.at[d, c], zsend.at[0], zrecv.at[d], {"z": near}).wait_recv()

                @pl.when(middle * d > 1)
                def _():
                    remote(whole.at[d, c], whole.at[5 - d, c], zsend.at[d + 2], zrecv.at[5 - d], {"z": near}).start()

                forward(d).start()

            forward(d).wait_recv()
        rows = own_ref.shape[0]
        inputs = whole[d].reshape(CORES * rows, -1)
        total = chunk(inputs, w_ref, f_ref[...], k_ref[...])
        part[d] = total.astype(jnp.bfloat16).reshape(part.shape[1:])
        handover(d).start()
        handover(d).wait_recv()

        @pl.when(d > 0)
        def _():
            both = part[d, c].astype(jnp.float32) + half[d].astype(jnp.float32)
            sums[d] = both.astype(jnp.bfloat16)

        @pl.when(d == 1)
        def _():
            to_near(1).start()

        @pl.when((1 - middle) * d > 1)
        def _():
            to_merge(d).start()

        return carry

    lax.fori_loop(0, depth, step, 0)
    if first:
        for d in range(depth):
            source = lax.rem(z - d + depth, depth)
            if d % 2 == 0:
                y_copies[d].wait_recv()
                block = block_place(m_ref, x, source, 1 - y, width)
                copy = remote(block, block, dsend.at[d], drecv.at[d], {"x": 1 - x})
            else:
                x_copies[d].wait_recv()
                block = block_place(m_ref, 1 - x, source, y, width)
                copy = remote(block, block, dsend.at[d], drecv.at[d], {"y": 1 - y})
            copy.start()
            d_copies.append(copy)

    @pl.when(middle == 1)
    def _():
        for d, leave in ((2, to_cross), (3, to_opposite)) if first else ((3, to_opposite), (2, to_cross)):
            remote(sums.at[d], extra.at[d], esend.at[d], erecv.at[d], {"z": near}).wait_recv()
            both = part[d, c].astype(jnp.float32) + half[d].astype(jnp.float32) + extra[d].astype(jnp.float32)
            sums[d] = both.astype(jnp.bfloat16)
            leave().start()

    total = part[0, c].astype(jnp.float32) + half[0].astype(jnp.float32)
    to_near(1).wait_recv()
    total = total + got[1].astype(jnp.float32)
    last = 2 + middle
    remote(sums.at[last], got.at[last], rsend.at[last], rrecv.at[last], {"z": near}).wait_recv()
    total = total + got[last].astype(jnp.float32)
    summed = RESIDUAL_SCALE * own_ref[...].astype(jnp.float32) + total * scale_ref[...]
    count = summed.shape[1]
    average = jnp.sum(summed, -1, keepdims=True) / count
    mean_square = jnp.sum(summed * summed, -1, keepdims=True) / count
    variance = mean_square - average * average
    normed = (summed - average) * lax.rsqrt(variance + EPSILON) * gain_ref[...] + shift_ref[...]
    if final:
        rows, columns = own_ref.shape[0], out_ref.shape[1]
        own_place = x * CORES + c
        here = pl.ds(pl.multiple_of(own_place * rows, rows), rows)
        sheet[...] = normed.astype(jnp.bfloat16)
        leaving = []
        for k, (tx, tc) in enumerate(((1 - x, c), (1 - x, 1 - c), (x, 1 - c))):
            there = pl.ds(pl.multiple_of((tx * CORES + tc) * columns, columns), columns)
            leaving.append(
                remote(sheet.at[:, there], out_ref.at[here], fsend.at[k], frecv.at[k], {"x": tx, "c": tc})
            )
            leaving[-1].start()
        out_ref[here] = sheet[:, pl.ds(pl.multiple_of(own_place * columns, columns), columns)]
        for copy in leaving:
            copy.wait()
    else:
        out_ref[...] = normed.astype(jnp.bfloat16)
    for d in range(depth):
        handover(d).wait_send()
        if d > 0:
            to_near(d).wait_send()
    if first:
        for d in range(depth):
            (x_copies if d % 2 == 0 else y_copies)[d].wait_recv()
            for copy in (y_copies[d], x_copies[d]):
                copy.wait_send()
            d_copies[d].wait()
            keeps[d].wait()
    else:
        beside.wait_send()
        for d in range(1, depth):
            forward(d).wait_send()
        line_waits(z, own_ref, lambda e: whole.at[e, c], zsend, zrecv)


def stage(depth, number, chunk, weights, factors, taps, own, scale, gain, shift, whole=None, held=None, final=False):
    rows, features = own.shape
    first = whole is not None
    dma = pltpu.SemaphoreType.DMA
    block = pltpu.VMEM((depth, rows, features), jnp.bfloat16)
    pair = pltpu.VMEM((depth, CORES, rows, features), jnp.bfloat16)
    operands = [weights, factors, taps, own, scale[None], gain[None], shift[None]]
    in_specs = [VMEM] * 7
    out_shape = [jax.ShapeDtypeStruct((rows, features), jnp.bfloat16)]
    out_specs = [VMEM]
    scratch = [pair, block, block, block, block] + [dma((depth,)) for _ in range(6)]
    if first:
        operands += [whole, held]
        in_specs += [VMEM, ANY]
        mats, part_rows, width = held.shape[1:]
        out_shape.append(jax.ShapeDtypeStruct((mats, 2, part_rows, depth * 2 * width), jnp.bfloat16))
        out_specs.append(ANY)
        scratch += [dma((depth,)) for _ in range(7)]
    else:
        scratch += [pair] + [dma((depth + 2,)) for _ in range(4)]
    if final:
        out_shape = [jax.ShapeDtypeStruct((2 * CORES * rows, features // (2 * CORES)), jnp.bfloat16)]
        scratch += [pltpu.VMEM((rows, features), jnp.bfloat16), dma((3,)), dma((3,))]
    return pl.pallas_call(
        functools.partial(stage_kernel, depth, chunk, first, final),
        out_shape=tuple(out_shape),
        in_specs=in_specs,
        out_specs=tuple(out_specs),
        scratch_shapes=scratch,
        compiler_params=pltpu.CompilerParams(
            collective_id=number, has_side_effects=True, vmem_limit_bytes=40 * 1024 * 1024
        ),
        name=f"stage_{number}",
    )(*operands)


def column_plan(
    depth, tokens, gate_weight, up_weight, down_weight, gate_scale, up_scale, down_scale,
    bgate_weight, cgate_weight, value_weight, bgate_scale, cgate_scale, value_scale, conv_taps,
    mixout_weight, mixout_scale, first_gain, first_shift, mixer_gain, mixer_shift, last_gain, last_shift,
):
    z, c = lax.axis_index("z"), lax.axis_index("c")
    own = lax.all_to_all(tokens, ("x", "c"), 0, 1, tiled=True)

    def cut(matrix):
        return matrix.astype(jnp.bfloat16).reshape(depth, -1, matrix.shape[1])

    blocks = jnp.stack([cut(gate_weight.T), cut(up_weight.T), cut(down_weight)], axis=1)
    mixer_blocks = jnp.stack(
        [cut(m.T) for m in (bgate_weight, cgate_weight, value_weight)] + [cut(mixout_weight)], axis=1
    )
    channels = bgate_weight.shape[1] // depth
    pieces = (gate_scale, up_scale, down_scale, bgate_scale, cgate_scale, value_scale, mixout_scale)
    flat = jnp.concatenate([piece.reshape(-1) for piece in pieces])
    flat = jnp.pad(flat, (0, -flat.shape[0] % 1024)).reshape(-1, 128)
    feed_weights, held, scales, whole = spread_weights(depth, blocks, mixer_blocks, flat, own)
    scales = scales.reshape(scales.shape[:4] + (-1,))
    mine = lax.dynamic_index_in_dim(lax.dynamic_index_in_dim(scales, c, 0, False), z, 2, False)
    edges = [0]
    for piece in pieces:
        edges.append(edges[-1] + piece.shape[1])

    def unit_scale(k):
        return mine[:, :, edges[k] : edges[k + 1]].reshape(-1)

    def feature_scale(k):
        return scales[..., edges[k] : edges[k + 1]].transpose(1, 0, 3, 2, 4).reshape(-1)

    feed_factors = jnp.stack([unit_scale(0), unit_scale(1)])
    mixer_factors = jnp.stack([unit_scale(3), unit_scale(4), unit_scale(5)])
    down_cols, mixout_cols = HALF_STEP * feature_scale(2), feature_scale(6)
    taps = conv_taps.reshape(TAPS, 2, CORES, depth, channels)
    taps = lax.dynamic_index_in_dim(lax.dynamic_index_in_dim(taps, c, 2, False), z, 2, False)
    taps = taps.reshape(TAPS, -1)

    first, mixer_weights = stage(
        depth, 1, feed_chunk, feed_weights, feed_factors, taps, own, down_cols, first_gain, first_shift, whole, held
    )
    (second,) = stage(
        depth, 2, mixer_chunk, mixer_weights, mixer_factors, taps, first, mixout_cols, mixer_gain, mixer_shift
    )
    (last,) = stage(
        depth, 3, feed_chunk, feed_weights, feed_factors, taps, second, down_cols, last_gain, last_shift, final=True
    )
    return last


def add_rows(gathered, shard_piece):
    return jnp.dot(gathered, shard_piece, preferred_element_type=jnp.float32)


def features(inputs):
    return lax.all_gather(inputs, "tp", axis=1, tiled=True)


def post_norm(residual, branch, norm_gain, norm_shift):
    summed = RESIDUAL_SCALE * residual.astype(jnp.float32) + branch
    moments = lax.psum((jnp.sum(summed, -1), jnp.sum(summed * summed, -1)), "tp")
    feature_total = summed.shape[1] * lax.axis_size("tp")
    average = (moments[0] / feature_total)[:, None]
    mean_square = (moments[1] / feature_total)[:, None]
    variance = mean_square - average * average
    return ((summed - average) * lax.rsqrt(variance + EPSILON) * norm_gain + norm_shift).astype(
        jnp.bfloat16
    )


def spread_back(weight_cols, left_rows):
    return (
        lax.psum_scatter(
            lax.dot_general(
                weight_cols, left_rows, (((0,), (1,)), ((), ())), preferred_element_type=jnp.float32
            ).astype(jnp.bfloat16),
            "tp",
            scatter_dimension=0,
            tiled=True,
        )
        .astype(jnp.float32)
        .T
    )


def shards(
    tokens,
    gate_weight,
    up_weight,
    down_weight,
    gate_scale,
    up_scale,
    down_scale,
    bgate_weight,
    cgate_weight,
    value_weight,
    bgate_scale,
    cgate_scale,
    value_scale,
    conv_taps,
    mixout_weight,
    mixout_scale,
    first_gain,
    first_shift,
    mixer_gain,
    mixer_shift,
    last_gain,
    last_shift,
):
    scales = (
        lax.all_gather(gate_scale, "fs", axis=1, tiled=True),
        lax.all_gather(up_scale, "fs", axis=1, tiled=True),
        lax.all_gather(down_scale, "fs", axis=1, tiled=True),
        lax.all_gather(bgate_scale, "fs", axis=1, tiled=True),
        lax.all_gather(cgate_scale, "fs", axis=1, tiled=True),
        lax.all_gather(value_scale, "fs", axis=1, tiled=True),
        lax.all_gather(mixout_scale, "fs", axis=1, tiled=True),
    )
    gate_cols, up_cols, down_cols, bgate_cols, cgate_cols, value_cols, mixout_cols = [
        scale_row.reshape(-1) for scale_row in scales
    ]
    tp_index = lax.axis_index("tp")
    columns = tokens.shape[1]

    def own_part(vector):
        return lax.dynamic_slice_in_dim(vector, tp_index * columns, columns)

    gate_low = gate_weight.astype(jnp.bfloat16)
    up_low = up_weight.astype(jnp.bfloat16)
    down_low = down_weight.astype(jnp.bfloat16)
    kept_gate, kept_up = (
        lax.all_gather(gate_low, "fs", axis=0, tiled=True),
        lax.all_gather(up_low, "fs", axis=0, tiled=True),
    )
    kept_down = lax.all_gather(down_low, "fs", axis=1, tiled=True)

    def channel_mix(gathered):
        gate_sum = jnp.dot(gathered, kept_gate, preferred_element_type=jnp.float32)
        up_sum = jnp.dot(gathered, kept_up, preferred_element_type=jnp.float32)
        hidden = (jax.nn.silu(gate_sum * gate_cols) * (up_sum * up_cols)).astype(jnp.bfloat16)
        return HALF_STEP * (spread_back(kept_down, hidden) * down_cols)

    first = post_norm(
        tokens, channel_mix(features(tokens)), own_part(first_gain), own_part(first_shift)
    )
    gathered = features(first)
    bgate_low = bgate_weight.astype(jnp.bfloat16)
    channels = bgate_low.shape[1]
    outgate = add_rows(gathered, lax.all_gather(bgate_low, "fs", axis=0, tiled=True))
    ingate = add_rows(
        gathered, lax.all_gather(cgate_weight.astype(jnp.bfloat16), "fs", axis=0, tiled=True)
    )
    values = add_rows(
        gathered, lax.all_gather(value_weight.astype(jnp.bfloat16), "fs", axis=0, tiled=True)
    )
    tap_weights = lax.dynamic_slice_in_dim(conv_taps, tp_index * channels, channels, 1)
    mixed = (ingate * cgate_cols * (values * value_cols)).reshape(-1, LENGTH, channels)
    padded = jnp.pad(mixed, ((0, 0), (TAPS - 1, 0), (0, 0)))
    convolved = jnp.zeros(mixed.shape, jnp.float32)
    for tap_index in range(TAPS):
        convolved = convolved + tap_weights[tap_index] * padded[:, tap_index : tap_index + LENGTH]
    gated = (outgate * bgate_cols * convolved.reshape(-1, channels)).astype(jnp.bfloat16)
    mix_full = lax.all_gather(mixout_weight.astype(jnp.bfloat16), "fs", axis=1, tiled=True)
    second = post_norm(
        first,
        spread_back(mix_full, gated) * mixout_cols,
        own_part(mixer_gain),
        own_part(mixer_shift),
    )
    return post_norm(
        second, channel_mix(features(second)), own_part(last_gain), own_part(last_shift)
    )


def solution(mesh):
    in_specs = (
        P("fs", "tp"),
        P("fs", "tp"),
        P("fs", "tp"),
        P("tp", "fs"),
        P("tp", "fs"),
        P("tp", "fs"),
        P("tp", "fs"),
        P("fs", "tp"),
        P("fs", "tp"),
        P("fs", "tp"),
        P("tp", "fs"),
        P("tp", "fs"),
        P("tp", "fs"),
        P(),
        P("tp", "fs"),
        P("tp", "fs"),
        P(),
        P(),
        P(),
        P(),
        P(),
        P(),
    )
    out_specs = P("fs", "tp")
    across = mesh.shape["tp"] // CORES
    if across == 2 and mesh.shape["fs"] == 8:
        depth = mesh.shape["fs"] // 2
        fine = Mesh(mesh.devices.reshape(depth, 2, 2, CORES), ("z", "y", "x", "c"))
        names = {"fs": ("z", "y"), "tp": ("x", "c")}

        def split(spec):
            return P(*(names.get(name) for name in spec))

        return jax.shard_map(
            functools.partial(column_plan, depth),
            mesh=fine,
            in_specs=tuple(split(spec) for spec in in_specs),
            out_specs=split(out_specs),
            check_vma=False,
        )
    return jax.shard_map(shards, mesh=mesh, in_specs=in_specs, out_specs=out_specs, check_vma=False)
```

```python
import functools

import jax
import jax.numpy as jnp
from jax import lax
from jax.experimental import pallas as pl
from jax.experimental.pallas import tpu as pltpu
from jax.sharding import Mesh
from jax.sharding import PartitionSpec as P

TAPS = 3
LENGTH = 128
CORES = 2

RESIDUAL_SCALE = 1.4142135623730951
HALF_STEP = 0.5
EPSILON = 1e-05
BY_AXIS = pl.DeviceIdType.MESH
ANY = pl.BlockSpec(memory_space=pl.ANY)
VMEM = pl.BlockSpec(memory_space=pltpu.VMEM)


def remote(src, dst, send, recv, target):
    return pltpu.make_async_remote_copy(
        src_ref=src, dst_ref=dst, send_sem=send, recv_sem=recv, device_id=target, device_id_type=BY_AXIS
    )


def dot_last(left, right):
    return lax.dot_general(left, right, (((1,), (1,)), ((), ())), preferred_element_type=jnp.float32)


def merged(ref, k):
    two, rows, features = ref.shape[1:]
    return ref[k].reshape(two * rows, features)


def feed_units(inputs, weights, factors, taps):
    gate_sum = dot_last(inputs, merged(weights, 0)) * factors[0:1]
    up_sum = dot_last(inputs, merged(weights, 1)) * factors[1:2]
    return (gate_sum / (1.0 + jnp.exp(-gate_sum)) * up_sum).astype(jnp.bfloat16)


def mixer_units(inputs, weights, factors, taps):
    outgate = dot_last(inputs, merged(weights, 0)) * factors[2:3]
    ingate = dot_last(inputs, merged(weights, 1)) * factors[3:4]
    values = dot_last(inputs, merged(weights, 2)) * factors[4:5]
    mixed = ingate * values
    position = lax.rem(lax.broadcasted_iota(jnp.int32, mixed.shape, 0), LENGTH)
    convolved = taps[TAPS - 1 : TAPS] * mixed
    for back in range(1, TAPS):
        earlier = jnp.where(position >= back, pltpu.roll(mixed, back, 0), 0.0)
        convolved = convolved + taps[TAPS - 1 - back : TAPS - back] * earlier
    return (outgate * convolved).astype(jnp.bfloat16)


def later_third(i):
    return i + (i // 2) * (5 - 2 * i)


def layer_kernel(
    tokens_ref, gate_ref, up_ref, down_ref, b_ref, c_ref, v_ref, mix_ref, *refs
):
    refs = list(refs)
    take = lambda n: [refs.pop(0) for _ in range(n)]
    scale_refs = take(7)
    taps_ref = take(1)[0]
    norms = [take(2) for _ in range(3)]
    (out_ref,) = take(1)
    tin, gate_full, up_full, down_full, *mixer_full = take(8)
    wsend, msend, feed_w, mixer_w, pack, blocks, lanes, units, channels, taps_own = take(10)
    own0, own1, own2, sheet = take(4)
    stages = [dict(zip(("whole", "part", "half", "sums", "extra", "got"), take(6))) for _ in range(3)]
    local, asend, arecv, ssend, srecv, fsend, frecv = take(7)
    zsend, zrecv, ysend, yrecv, xsend, xrecv, dsend, drecv = take(8)
    mzsend, mzrecv, mysend, myrecv, mxsend, mxrecv, mdsend, mdrecv = take(8)
    for state in stages:
        names = ("rs", "rr", "ls", "lr", "cs", "cr", "hs", "hr", "ps", "gr", "er")
        state.update(zip(names, take(len(names))))

    z, y, x, c = (lax.axis_index(axis) for axis in ("z", "y", "x", "c"))
    near = z + 1 - 2 * lax.rem(z, 2)
    cross = lax.rem(z + 2, 4)
    opposite = 3 - z
    middle = lax.rem((z + 1) // 2, 2)
    partner = (z, near, cross, opposite)
    to_x, to_y, to_c = {"x": 1 - x}, {"y": 1 - y}, {"c": 1 - c}

    def partner_of(e):
        odd = 1 - 2 * lax.rem(z, 2)
        return lax.rem(z + odd * lax.rem(e, 2) + 2 * (e // 2), 4)

    loads = [
        pltpu.make_async_copy(src, dst, local.at[k])
        for k, (src, dst) in enumerate(
            zip(
                (tokens_ref, down_ref, gate_ref, up_ref, b_ref, c_ref, v_ref, mix_ref),
                (tin, down_full, gate_full, up_full, *mixer_full),
            )
        )
    ]
    for load in loads:
        load.start()
    barrier = pltpu.get_barrier_semaphore()
    greeted = [{"z": t} for t in partner[1:]] + [to_x, to_y, to_c, {"x": 1 - x, "c": 1 - c}]
    for target in greeted:
        pl.semaphore_signal(barrier, inc=1, device_id=target, device_id_type=BY_AXIS)
    pack[...] = jnp.zeros_like(pack)
    for k, scale_ref in enumerate(scale_refs):
        pack[k : k + 1, 0 : scale_ref.shape[1]] = scale_ref[...]
    pl.semaphore_wait(barrier, len(greeted))

    rows, features = own0.shape
    columns = tin.shape[1]
    place_here = x * CORES + c

    def strip(t, width):
        return pl.ds(pl.multiple_of(t * width, width), width)

    loads[0].wait()
    trades = []
    for k, (tx, tc) in enumerate(((1 - x, c), (1 - x, 1 - c), (x, 1 - c))):
        trades.append(
            remote(
                tin.at[strip(tx * CORES + tc, rows)],
                own0.at[:, strip(place_here, columns)],
                asend.at[k],
                arecv.at[k],
                {"x": tx, "c": tc},
            )
        )
        trades[-1].start()
    own0[:, strip(place_here, columns)] = tin[strip(place_here, rows)]

    hidden_rows, width = feed_w.shape[2], wsend.shape[2]
    channel_rows = mixer_w.shape[2]

    def place(p, px, pz, py):
        return feed_w.at[p, px, :, strip(pz * 2 + py, width)]

    def y_copy(e, p, src=None):
        dst = place(p, x, partner[e], y)
        return remote(dst if src is None else src, dst, ysend.at[e * 3 + p], yrecv.at[e * 3 + p], to_y)

    def x_copy(e, p, src=None):
        dst = place(p, x, partner[e], y)
        return remote(dst if src is None else src, dst, xsend.at[e * 3 + p], xrecv.at[e * 3 + p], to_x)

    def z_copy(e, p):
        src = wsend.at[p, strip(partner[e], hidden_rows)]
        return remote(src, place(p, x, z, y), zsend.at[e * 3 + p], zrecv.at[e * 3 + p], {"z": partner[e]})

    def z_landed(e, p):
        dst = place(p, x, partner[e], y)
        return remote(dst, dst, zsend.at[e * 3 + p], zrecv.at[e * 3 + p], {"z": partner[e]})

    def d_copy(e, p):
        k = e * 3 + p
        if (e + p) % 2 == 0:
            block = place(p, x, partner[e], 1 - y)
            return remote(block, block, dsend.at[k], drecv.at[k], to_x)
        block = place(p, 1 - x, partner[e], y)
        return remote(block, block, dsend.at[k], drecv.at[k], to_y)

    def relay(e, p):
        (y_copy if (e + p) % 2 == 0 else x_copy)(e, p).wait_recv()
        d_copy(e, p).start()

    def turned(src, dst, p):
        def turn(j, carry):
            here = strip(j, 128)
            dst[p, here, :] = src[:, here].T.astype(jnp.bfloat16)
            return carry

        lax.fori_loop(0, src.shape[1] // 128, turn, 0)

    order = (2, 0, 1)
    for p, full in zip(order, (down_full, gate_full, up_full)):
        loads[(2, 3, 1)[p]].wait()
        if p == 2:
            wsend[p] = full[...].astype(jnp.bfloat16)
        else:
            turned(full, wsend, p)
        mine = wsend.at[p, strip(z, hidden_rows)]
        y_copy(0, p, mine).start()
        x_copy(0, p, mine).start()
        for e in (1, 3, 2):
            z_copy(e, p).start()
    for p in order:
        feed_w[p, x, :, strip(z * 2 + y, width)] = wsend[p, strip(z, hidden_rows)]

    scale_sends = []
    for e in (1, 2, 3):
        scale_sends.append(remote(pack, blocks.at[c, x, y, z], ssend.at[e], srecv.at[e], {"z": partner[e]}))
        scale_sends[-1].start()
    blocks[c, x, y, z] = pack[...]

    def piece(state, s, h):
        return state["whole"].at[s, c, pl.ds(h * (rows // 2), rows // 2)]

    def spread(state, own):
        state["own"] = own
        for h in range(2):
            src = own.at[pl.ds(h * (rows // 2), rows // 2)]

            @pl.when(z < 3)
            def _():
                remote(src, piece(state, z, h), state["rs"].at[h], state["rr"].at[2 + h], {"z": z + 1}).start()

            @pl.when(z > 0)
            def _():
                remote(src, piece(state, z, h), state["ls"].at[h], state["lr"].at[2 + h], {"z": z - 1}).start()

        for h in range(2):
            src = own.at[pl.ds(h * (rows // 2), rows // 2)]
            remote(src, piece(state, z, h), state["cs"].at[z * 2 + h], state["cr"].at[z * 2 + h], to_c).start()
        state["whole"][z, c] = own[...]

    def beside(state, s, h):
        src = piece(state, s, h)
        return remote(src, src, state["cs"].at[s * 2 + h], state["cr"].at[s * 2 + h], to_c)

    def pass_on(state, k, h):
        slot = k * 2 + h

        @pl.when(z >= k)
        def _():
            s = lax.rem(z - k + 4, 4)
            src = piece(state, s, h)
            remote(src, src, state["rs"].at[slot], state["rr"].at[slot], to_c).wait_recv()

            @pl.when(z < 3)
            def _():
                remote(src, src, state["rs"].at[slot], state["rr"].at[slot + 2], {"z": z + 1}).start()

            beside(state, s, h).start()

        @pl.when(z + k < 4)
        def _():
            s = lax.rem(z + k, 4)
            src = piece(state, s, h)
            remote(src, src, state["ls"].at[slot], state["lr"].at[slot], to_c).wait_recv()

            @pl.when(z > 0)
            def _():
                remote(src, src, state["ls"].at[slot], state["lr"].at[slot + 2], {"z": z - 1}).start()

            beside(state, s, h).start()

    def spread_done(state):
        for k in range(4):
            for h in range(2):
                slot = k * 2 + h
                src = piece(state, z, h)

                @pl.when((z >= k) & (z < 3))
                def _():
                    remote(src, src, state["rs"].at[slot], state["rr"].at[slot], to_c).wait_send()

                @pl.when((z + k < 4) & (z > 0))
                def _():
                    remote(src, src, state["ls"].at[slot], state["lr"].at[slot], to_c).wait_send()

                beside(state, k, h).wait_send()

    for k, full in enumerate(mixer_full):
        loads[4 + k].wait()
        if k == 3:
            msend[k] = full[...].astype(jnp.bfloat16)
        else:
            turned(full, msend, k)
    for copy in trades:
        copy.wait_recv()
    spread(stages[0], own0)

    def m_place(px, pz, py):
        return mixer_w.at[:, px, :, strip(pz * 2 + py, width)]

    def m_y(e, src=None):
        dst = m_place(x, partner_of(e), y)
        return remote(dst if src is None else src, dst, mysend.at[e], myrecv.at[e], to_y)

    def m_x(e, src=None):
        dst = m_place(x, partner_of(e), y)
        return remote(dst if src is None else src, dst, mxsend.at[e], mxrecv.at[e], to_x)

    def m_z(e):
        src = msend.at[:, strip(partner_of(e), channel_rows)]
        return remote(src, m_place(x, z, y), mzsend.at[e], mzrecv.at[e], {"z": partner_of(e)})

    def m_d(e):
        if e % 2 == 0:
            block = m_place(x, partner[e], 1 - y)
            return remote(block, block, mdsend.at[e], mdrecv.at[e], to_x)
        block = m_place(1 - x, partner[e], y)
        return remote(block, block, mdsend.at[e], mdrecv.at[e], to_y)

    def m_relay(e):
        (m_y if e % 2 == 0 else m_x)(e).wait_recv()
        m_d(e).start()

    hops = [
        remote(part, part, ssend.at[slot], srecv.at[slot], target)
        for slot, (part, target) in zip(
            (0, 4, 5), ((blocks.at[c, x, y], to_y), (blocks.at[c, x], to_x), (blocks.at[c], to_c))
        )
    ]
    sent = [(0, p) for p in order]
    arriving = [(e, p) for p in order for e in (1, 3, 2)]
    for j, (e, p) in enumerate(arriving):
        z_landed(e, p).wait_recv()
        y_copy(e, p).start()
        x_copy(e, p).start()
        sent.append((e, p))
        relay(*sent[j])
        if j == 2:
            for copy in scale_sends:
                copy.wait_recv()
            hops[0].start()
        if j in (4, 6):
            hops[j // 2 - 2].wait_recv()
            hops[j // 2 - 1].start()
    for k in range(1, 4):
        for h in range(2):
            pass_on(stages[0], k, h)
    for e in (1, 3, 2):
        m_z(e).start()
    mine = msend.at[:, strip(z, channel_rows)]
    mixer_w[:, x, :, strip(z * 2 + y, width)] = msend[:, strip(z, channel_rows)]
    hops[2].wait_recv()

    wide = units.shape[1]
    unit_total = jnp.zeros(units.shape, jnp.float32)
    channel_total = jnp.zeros(channels.shape, jnp.float32)
    unit_part = scale_refs[0].shape[1]
    lane_part = scale_refs[2].shape[1]
    for px in range(2):
        for py in range(2):
            block = blocks[c, px, py, z]
            padded = jnp.concatenate([block, jnp.zeros((block.shape[0], wide - block.shape[1]), jnp.float32)], 1)
            k = px * 2 + py
            unit_total = unit_total + (pltpu.roll(padded, k * unit_part, 1) if k else padded)
            channel_total = channel_total + (pltpu.roll(block, k * lane_part, 1) if k else block)
    units[...] = unit_total
    channels[...] = channel_total
    pair = 2 * lane_part
    for px in range(2):
        for pc in range(CORES):
            for pz in range(4):
                low, high = (blocks[pc, px, py, pz][:, 0:pair] for py in range(2))
                start = ((px * CORES + pc) * 4 + pz) * pair
                lanes[:, start : start + pair] = low + pltpu.roll(high, lane_part, 1)
    for px in range(2):
        taps_own[:, px * pair : (px + 1) * pair] = taps_ref[:, strip((px * CORES + c) * 4 + z, pair)]

    for e, p in sent[len(arriving) :]:
        relay(e, p)
    m_y(0, mine).start()
    m_x(0, mine).start()
    for e, p in sent:
        (x_copy if (e + p) % 2 == 0 else y_copy)(e, p).wait_recv()
        d_copy(e, p).wait_recv()

    half_width = features // 2

    def to_near(state, e, h):
        return remote(
            state["sums"].at[e, h], state["got"].at[0, h], state["ps"].at[e * 2 + h], state["gr"].at[h], {"z": near}
        )

    def to_merge(state, e, h):
        slot = (5 - e) * 2 + h
        return remote(
            state["sums"].at[e, h], state["extra"].at[5 - e, h], state["ps"].at[e * 2 + h], state["er"].at[slot], {"z": near}
        )

    def to_far(state, e, h):
        return remote(
            state["sums"].at[e, h], state["got"].at[1, h], state["ps"].at[e * 2 + h], state["gr"].at[2 + h],
            {"z": partner[e]},
        )

    def handover(state, e, h):
        return remote(
            state["part"].at[e, h, 1 - c], state["half"].at[e, h], state["hs"].at[e * 2 + h], state["hr"].at[e * 2 + h], to_c
        )

    def run(number, units_of, weights, factors, before, pick):
        state = stages[number]
        exit_k = weights.shape[0] - 1

        def step(i, carry):
            before(i)
            e = pick(i)
            s = partner_of(e)
            for h in range(2):
                beside(state, s, h).wait_recv()
            inputs = state["whole"][s].reshape(CORES * rows, features)
            hidden = units_of(inputs, weights, factors, taps_own[...])
            for h in range(2):
                last = weights[exit_k, :, :, pl.ds(h * half_width, half_width)].reshape(-1, half_width)
                total = jnp.dot(hidden, last, preferred_element_type=jnp.float32)
                state["part"][e, h] = total.astype(jnp.bfloat16).reshape(CORES, rows, half_width)
                handover(state, e, h).start()
            for h in range(2):
                handover(state, e, h).wait_recv()
                both = state["part"][e, h, c].astype(jnp.float32) + state["half"][e, h].astype(jnp.float32)
                state["sums"][e, h] = both.astype(jnp.bfloat16)

                @pl.when(e == 1)
                def _():
                    to_near(state, 1, h).start()

                @pl.when((1 - middle) * e > 1)
                def _():
                    to_merge(state, e, h).start()

            return carry

        lax.fori_loop(0, 4, step, 0)

        @pl.when(middle == 1)
        def _():
            for e in (2, 3) if number == 0 else (3, 2):
                for h in range(2):
                    far = state["extra"].at[e, h]
                    remote(far, far, state["ps"].at[e * 2 + h], state["er"].at[e * 2 + h], to_c).wait_recv()
                    both = state["sums"][e, h].astype(jnp.float32) + state["extra"][e, h].astype(jnp.float32)
                    state["sums"][e, h] = both.astype(jnp.bfloat16)
                    to_far(state, e, h).start()

    def finish(number, out, factor):
        state = stages[number]
        own = state["own"]
        gain_ref, shift_ref = norms[number]
        scale_row = 6 if number == 1 else 5
        pieces, one, two = [], 0.0, 0.0
        for h in range(2):
            cols = slice(h * half_width, (h + 1) * half_width)
            total = state["sums"][0, h].astype(jnp.float32)
            for k in range(2):
                src = state["got"].at[k, h]
                remote(src, src, state["ps"].at[h], state["gr"].at[k * 2 + h], to_c).wait_recv()
                total = total + state["got"][k, h].astype(jnp.float32)
            scale = lanes[scale_row : scale_row + 1, cols] * factor
            summed = RESIDUAL_SCALE * own[:, cols].astype(jnp.float32) + total * scale
            pieces.append(summed)
            one = one + jnp.sum(summed, -1, keepdims=True)
            two = two + jnp.sum(summed * summed, -1, keepdims=True)
        average = one / features
        variance = two / features - average * average
        inverse = lax.rsqrt(variance + EPSILON)
        for h in range(2):
            cols = slice(h * half_width, (h + 1) * half_width)
            normed = (pieces[h] - average) * inverse * gain_ref[:, cols] + shift_ref[:, cols]
            out[:, cols] = normed.astype(jnp.bfloat16)

    def mixer_arrivals(i):
        @pl.when(i > 0)
        def _():
            e = later_third(i)
            landed = m_place(x, partner_of(e), y)
            remote(landed, landed, mzsend.at[e], mzrecv.at[e], to_c).wait_recv()
            m_y(e).start()
            m_x(e).start()

    def line_arrivals(state):
        def before(i):
            @pl.when(i == 1)
            def _():
                for h in range(2):
                    pass_on(state, 1, h)

            @pl.when(i == 2)
            def _():
                pass_on(state, 2, 0)

            @pl.when(i == 2 + middle)
            def _():
                pass_on(state, 2, 1)

            @pl.when(i == 3)
            def _():
                for h in range(2):
                    pass_on(state, 3, h)

        return before

    run(
        0, feed_units, feed_w, units[:, : 2 * hidden_rows], mixer_arrivals,
        lambda i: (1 - middle) * (3 - i) + middle * lax.rem(i + 1, 4),
    )
    m_relay(0)
    m_relay(1)
    finish(0, own1, HALF_STEP)
    spread(stages[1], own1)
    m_relay(3)
    m_relay(2)
    for e in range(4):
        (m_x if e % 2 == 0 else m_y)(e).wait_recv()
        m_d(e).wait_recv()

    def arrival_order(i):
        return (1 - middle) * i + middle * ((i + 2) // 3) * (lax.rem(i + 1, 3) + 1)

    run(1, mixer_units, mixer_w, channels[...], line_arrivals(stages[1]), arrival_order)
    finish(1, own2, 1.0)
    spread(stages[2], own2)
    run(2, feed_units, feed_w, units[:, : 2 * hidden_rows], line_arrivals(stages[2]), arrival_order)
    finish(2, sheet, HALF_STEP)

    here = strip(place_here, rows)
    leaving = []
    for k, (tx, tc) in enumerate(((1 - x, c), (1 - x, 1 - c), (x, 1 - c))):
        there = strip(tx * CORES + tc, columns)
        leaving.append(
            remote(sheet.at[:, there], out_ref.at[here], fsend.at[k], frecv.at[k], {"x": tx, "c": tc})
        )
        leaving[-1].start()
    out_ref[here] = sheet[:, strip(place_here, columns)]

    for copy in trades + scale_sends + hops:
        copy.wait_send()
    for e, p in sent:
        y_copy(e, p).wait_send()
        x_copy(e, p).wait_send()
        d_copy(e, p).wait_send()
        if e > 0:
            z_copy(e, p).wait_send()
    for e in range(4):
        m_y(e).wait_send()
        m_x(e).wait_send()
        m_d(e).wait_send()
        if e > 0:
            m_z(e).wait_send()
    for state in stages:
        spread_done(state)
        for e in range(4):
            for h in range(2):
                handover(state, e, h).wait_send()
                if e > 0:
                    to_near(state, e, h).wait_send()
    for copy in leaving:
        copy.wait()


def column_plan(
    depth, tokens, gate_weight, up_weight, down_weight, gate_scale, up_scale, down_scale,
    bgate_weight, cgate_weight, value_weight, bgate_scale, cgate_scale, value_scale, conv_taps,
    mixout_weight, mixout_scale, first_gain, first_shift, mixer_gain, mixer_shift, last_gain, last_shift,
):
    dma = pltpu.SemaphoreType.DMA
    low, full = jnp.bfloat16, jnp.float32
    rows = tokens.shape[0] // (2 * CORES)
    features = tokens.shape[1] * 2 * CORES
    half_width = features // 2
    width = gate_weight.shape[0]
    hidden = gate_weight.shape[1]
    channels = bgate_weight.shape[1]
    lanes = max(-(-gate_scale.shape[1] // 128) * 128, 4 * bgate_scale.shape[1])
    big = [gate_weight, up_weight, down_weight, bgate_weight, cgate_weight, value_weight, mixout_weight]
    scales = [gate_scale, up_scale, bgate_scale, cgate_scale, value_scale, down_scale, mixout_scale]
    vectors = [first_gain, first_shift, mixer_gain, mixer_shift, last_gain, last_shift]
    operands = [tokens, *big, *scales, conv_taps] + [v[None] for v in vectors]
    scratch = [pltpu.VMEM(tokens.shape, low)] + [pltpu.VMEM(w.shape, full) for w in big]
    scratch += [
        pltpu.VMEM((3, hidden, width), low),
        pltpu.VMEM((4, channels, width), low),
        pltpu.VMEM((3, 2, hidden // depth, features), low),
        pltpu.VMEM((4, 2, channels // depth, features), low),
        pltpu.VMEM((8, lanes), full),
        pltpu.VMEM((CORES, 2, 2, depth, 8, lanes), full),
        pltpu.VMEM((8, features), full),
        pltpu.VMEM((8, -(-2 * hidden // depth // 128) * 128), full),
        pltpu.VMEM((8, 2 * channels // depth), full),
        pltpu.VMEM((TAPS, 2 * channels // depth), full),
    ]
    scratch += [pltpu.VMEM((rows, features), low) for _ in range(4)]
    for _ in range(3):
        scratch += [
            pltpu.VMEM((depth, CORES, rows, features), low),
            pltpu.VMEM((depth, 2, CORES, rows, half_width), low),
            pltpu.VMEM((depth, 2, rows, half_width), low),
            pltpu.VMEM((depth, 2, rows, half_width), low),
            pltpu.VMEM((depth, 2, rows, half_width), low),
            pltpu.VMEM((2, 2, rows, half_width), low),
        ]
    scratch += [dma((8,)), dma((3,)), dma((3,)), dma((6,)), dma((6,)), dma((3,)), dma((3,))]
    scratch += [dma((12,)) for _ in range(8)]
    scratch += [dma((4,)) for _ in range(8)]
    for _ in range(3):
        scratch += [dma((10,)) for _ in range(4)] + [dma((8,)) for _ in range(7)]
    return pl.pallas_call(
        layer_kernel,
        out_shape=jax.ShapeDtypeStruct(tokens.shape, low),
        in_specs=[ANY] * 8 + [VMEM] * (len(operands) - 8),
        out_specs=VMEM,
        scratch_shapes=scratch,
        compiler_params=pltpu.CompilerParams(
            collective_id=0, has_side_effects=True, vmem_limit_bytes=60 * 1024 * 1024
        ),
        name="layer",
    )(*operands)


def add_rows(gathered, shard_piece):
    return jnp.dot(gathered, shard_piece, preferred_element_type=jnp.float32)


def features(inputs):
    return lax.all_gather(inputs, "tp", axis=1, tiled=True)


def post_norm(residual, branch, norm_gain, norm_shift):
    summed = RESIDUAL_SCALE * residual.astype(jnp.float32) + branch
    moments = lax.psum((jnp.sum(summed, -1), jnp.sum(summed * summed, -1)), "tp")
    feature_total = summed.shape[1] * lax.axis_size("tp")
    average = (moments[0] / feature_total)[:, None]
    mean_square = (moments[1] / feature_total)[:, None]
    variance = mean_square - average * average
    return ((summed - average) * lax.rsqrt(variance + EPSILON) * norm_gain + norm_shift).astype(
        jnp.bfloat16
    )


def spread_back(weight_cols, left_rows):
    return (
        lax.psum_scatter(
            lax.dot_general(
                weight_cols, left_rows, (((0,), (1,)), ((), ())), preferred_element_type=jnp.float32
            ).astype(jnp.bfloat16),
            "tp",
            scatter_dimension=0,
            tiled=True,
        )
        .astype(jnp.float32)
        .T
    )


def shards(
    tokens,
    gate_weight,
    up_weight,
    down_weight,
    gate_scale,
    up_scale,
    down_scale,
    bgate_weight,
    cgate_weight,
    value_weight,
    bgate_scale,
    cgate_scale,
    value_scale,
    conv_taps,
    mixout_weight,
    mixout_scale,
    first_gain,
    first_shift,
    mixer_gain,
    mixer_shift,
    last_gain,
    last_shift,
):
    scales = (
        lax.all_gather(gate_scale, "fs", axis=1, tiled=True),
        lax.all_gather(up_scale, "fs", axis=1, tiled=True),
        lax.all_gather(down_scale, "fs", axis=1, tiled=True),
        lax.all_gather(bgate_scale, "fs", axis=1, tiled=True),
        lax.all_gather(cgate_scale, "fs", axis=1, tiled=True),
        lax.all_gather(value_scale, "fs", axis=1, tiled=True),
        lax.all_gather(mixout_scale, "fs", axis=1, tiled=True),
    )
    gate_cols, up_cols, down_cols, bgate_cols, cgate_cols, value_cols, mixout_cols = [
        scale_row.reshape(-1) for scale_row in scales
    ]
    tp_index = lax.axis_index("tp")
    columns = tokens.shape[1]

    def own_part(vector):
        return lax.dynamic_slice_in_dim(vector, tp_index * columns, columns)

    gate_low = gate_weight.astype(jnp.bfloat16)
    up_low = up_weight.astype(jnp.bfloat16)
    down_low = down_weight.astype(jnp.bfloat16)
    kept_gate, kept_up = (
        lax.all_gather(gate_low, "fs", axis=0, tiled=True),
        lax.all_gather(up_low, "fs", axis=0, tiled=True),
    )
    kept_down = lax.all_gather(down_low, "fs", axis=1, tiled=True)

    def channel_mix(gathered):
        gate_sum = jnp.dot(gathered, kept_gate, preferred_element_type=jnp.float32)
        up_sum = jnp.dot(gathered, kept_up, preferred_element_type=jnp.float32)
        hidden = (jax.nn.silu(gate_sum * gate_cols) * (up_sum * up_cols)).astype(jnp.bfloat16)
        return HALF_STEP * (spread_back(kept_down, hidden) * down_cols)

    first = post_norm(
        tokens, channel_mix(features(tokens)), own_part(first_gain), own_part(first_shift)
    )
    gathered = features(first)
    bgate_low = bgate_weight.astype(jnp.bfloat16)
    channels = bgate_low.shape[1]
    outgate = add_rows(gathered, lax.all_gather(bgate_low, "fs", axis=0, tiled=True))
    ingate = add_rows(
        gathered, lax.all_gather(cgate_weight.astype(jnp.bfloat16), "fs", axis=0, tiled=True)
    )
    values = add_rows(
        gathered, lax.all_gather(value_weight.astype(jnp.bfloat16), "fs", axis=0, tiled=True)
    )
    tap_weights = lax.dynamic_slice_in_dim(conv_taps, tp_index * channels, channels, 1)
    mixed = (ingate * cgate_cols * (values * value_cols)).reshape(-1, LENGTH, channels)
    padded = jnp.pad(mixed, ((0, 0), (TAPS - 1, 0), (0, 0)))
    convolved = jnp.zeros(mixed.shape, jnp.float32)
    for tap_index in range(TAPS):
        convolved = convolved + tap_weights[tap_index] * padded[:, tap_index : tap_index + LENGTH]
    gated = (outgate * bgate_cols * convolved.reshape(-1, channels)).astype(jnp.bfloat16)
    mix_full = lax.all_gather(mixout_weight.astype(jnp.bfloat16), "fs", axis=1, tiled=True)
    second = post_norm(
        first,
        spread_back(mix_full, gated) * mixout_cols,
        own_part(mixer_gain),
        own_part(mixer_shift),
    )
    return post_norm(
        second, channel_mix(features(second)), own_part(last_gain), own_part(last_shift)
    )


def solution(mesh):
    in_specs = (
        P("fs", "tp"),
        P("fs", "tp"),
        P("fs", "tp"),
        P("tp", "fs"),
        P("tp", "fs"),
        P("tp", "fs"),
        P("tp", "fs"),
        P("fs", "tp"),
        P("fs", "tp"),
        P("fs", "tp"),
        P("tp", "fs"),
        P("tp", "fs"),
        P("tp", "fs"),
        P(),
        P("tp", "fs"),
        P("tp", "fs"),
        P(),
        P(),
        P(),
        P(),
        P(),
        P(),
    )
    out_specs = P("fs", "tp")
    across = mesh.shape["tp"] // CORES
    if across == 2 and mesh.shape["fs"] == 8:
        depth = mesh.shape["fs"] // 2
        fine = Mesh(mesh.devices.reshape(depth, 2, 2, CORES), ("z", "y", "x", "c"))
        names = {"fs": ("z", "y"), "tp": ("x", "c")}

        def split(spec):
            return P(*(names.get(name) for name in spec))

        return jax.shard_map(
            functools.partial(column_plan, depth),
            mesh=fine,
            in_specs=tuple(split(spec) for spec in in_specs),
            out_specs=split(out_specs),
            check_vma=False,
        )
    return jax.shard_map(shards, mesh=mesh, in_specs=in_specs, out_specs=out_specs, check_vma=False)
```

```python
import functools

import jax
import jax.numpy as jnp
from jax import lax
from jax.experimental import pallas as pl
from jax.experimental.pallas import tpu as pltpu
from jax.sharding import Mesh
from jax.sharding import PartitionSpec as P

TAPS = 3
LENGTH = 128
CORES = 2

RESIDUAL_SCALE = 1.4142135623730951
HALF_STEP = 0.5
EPSILON = 1e-05
BY_AXIS = pl.DeviceIdType.MESH
ANY = pl.BlockSpec(memory_space=pl.ANY)
VMEM = pl.BlockSpec(memory_space=pltpu.VMEM)


def remote(src, dst, send, recv, target):
    return pltpu.make_async_remote_copy(
        src_ref=src, dst_ref=dst, send_sem=send, recv_sem=recv, device_id=target, device_id_type=BY_AXIS
    )


def dot_last(left, right):
    return lax.dot_general(left, right, (((1,), (1,)), ((), ())), preferred_element_type=jnp.float32)


def merged(ref, k):
    two, rows, features = ref.shape[1:]
    return ref[k].reshape(two * rows, features)


def feed_units(inputs, weights, factors, taps):
    gate_sum = dot_last(inputs, merged(weights, 0)) * factors[0:1]
    up_sum = dot_last(inputs, merged(weights, 1)) * factors[1:2]
    return (gate_sum / (1.0 + jnp.exp(-gate_sum)) * up_sum).astype(jnp.bfloat16)


def mixer_units(inputs, weights, factors, taps):
    outgate = dot_last(inputs, merged(weights, 0)) * factors[2:3]
    ingate = dot_last(inputs, merged(weights, 1)) * factors[3:4]
    values = dot_last(inputs, merged(weights, 2)) * factors[4:5]
    mixed = ingate * values
    position = lax.rem(lax.broadcasted_iota(jnp.int32, mixed.shape, 0), LENGTH)
    convolved = taps[TAPS - 1 : TAPS] * mixed
    for back in range(1, TAPS):
        earlier = jnp.where(position >= back, pltpu.roll(mixed, back, 0), 0.0)
        convolved = convolved + taps[TAPS - 1 - back : TAPS - back] * earlier
    return (outgate * convolved).astype(jnp.bfloat16)


def later_third(i):
    return i + (i // 2) * (5 - 2 * i)


def layer_kernel(
    tokens_ref, gate_ref, up_ref, down_ref, b_ref, c_ref, v_ref, mix_ref, *refs
):
    refs = list(refs)
    take = lambda n: [refs.pop(0) for _ in range(n)]
    scale_refs = take(7)
    taps_ref = take(1)[0]
    norms = [take(2) for _ in range(3)]
    (out_ref,) = take(1)
    tin, gate_full, up_full, down_full, *mixer_full = take(8)
    wsend, msend, feed_w, mixer_w, pack, blocks, lanes, units, channels, taps_own = take(10)
    own0, own1, own2, sheet = take(4)
    stages = [dict(zip(("whole", "part", "half", "sums", "extra", "got"), take(6))) for _ in range(3)]
    local, asend, arecv, ssend, srecv, fsend, frecv = take(7)
    zsend, zrecv, ysend, yrecv, xsend, xrecv, dsend, drecv = take(8)
    mzsend, mzrecv, mysend, myrecv, mxsend, mxrecv, mdsend, mdrecv = take(8)
    for state in stages:
        names = ("rs", "rr", "ls", "lr", "cs", "cr", "hs", "hr", "ps", "gr", "er")
        state.update(zip(names, take(len(names))))

    z, y, x, c = (lax.axis_index(axis) for axis in ("z", "y", "x", "c"))
    near = z + 1 - 2 * lax.rem(z, 2)
    cross = lax.rem(z + 2, 4)
    opposite = 3 - z
    middle = lax.rem((z + 1) // 2, 2)
    partner = (z, near, cross, opposite)
    to_x, to_y, to_c = {"x": 1 - x}, {"y": 1 - y}, {"c": 1 - c}

    def partner_of(e):
        odd = 1 - 2 * lax.rem(z, 2)
        return lax.rem(z + odd * lax.rem(e, 2) + 2 * (e // 2), 4)

    loads = [
        pltpu.make_async_copy(src, dst, local.at[k])
        for k, (src, dst) in enumerate(
            zip(
                (tokens_ref, down_ref, gate_ref, up_ref, b_ref, c_ref, v_ref, mix_ref),
                (tin, down_full, gate_full, up_full, *mixer_full),
            )
        )
    ]
    for load in loads:
        load.start()
    barrier = pltpu.get_barrier_semaphore()
    greeted = [{"z": t} for t in partner[1:]] + [to_x, to_y, to_c, {"x": 1 - x, "c": 1 - c}]
    for target in greeted:
        pl.semaphore_signal(barrier, inc=1, device_id=target, device_id_type=BY_AXIS)
    pack[...] = jnp.zeros_like(pack)
    for k, scale_ref in enumerate(scale_refs):
        pack[k : k + 1, 0 : scale_ref.shape[1]] = scale_ref[...]
    pl.semaphore_wait(barrier, len(greeted))

    scale_sends = []
    for e in (1, 2, 3):
        scale_sends.append(remote(pack, blocks.at[c, x, y, z], ssend.at[e], srecv.at[e], {"z": partner[e]}))
        scale_sends[-1].start()
    blocks[c, x, y, z] = pack[...]

    rows, features = own0.shape
    columns = tin.shape[1]
    place_here = x * CORES + c

    def strip(t, width):
        return pl.ds(pl.multiple_of(t * width, width), width)

    loads[0].wait()
    trades = []
    for k, (tx, tc) in enumerate(((1 - x, c), (1 - x, 1 - c), (x, 1 - c))):
        trades.append(
            remote(
                tin.at[strip(tx * CORES + tc, rows)],
                own0.at[:, strip(place_here, columns)],
                asend.at[k],
                arecv.at[k],
                {"x": tx, "c": tc},
            )
        )
        trades[-1].start()
    own0[:, strip(place_here, columns)] = tin[strip(place_here, rows)]

    hidden_rows, width = feed_w.shape[2], wsend.shape[2]
    channel_rows = mixer_w.shape[2]

    def place(p, px, pz, py):
        return feed_w.at[p, px, :, strip(pz * 2 + py, width)]

    def y_copy(e, p, src=None):
        dst = place(p, x, partner[e], y)
        return remote(dst if src is None else src, dst, ysend.at[e * 3 + p], yrecv.at[e * 3 + p], to_y)

    def x_copy(e, p, src=None):
        dst = place(p, x, partner[e], y)
        return remote(dst if src is None else src, dst, xsend.at[e * 3 + p], xrecv.at[e * 3 + p], to_x)

    def z_copy(e, p):
        src = wsend.at[p, strip(partner[e], hidden_rows)]
        return remote(src, place(p, x, z, y), zsend.at[e * 3 + p], zrecv.at[e * 3 + p], {"z": partner[e]})

    def z_landed(e, p):
        dst = place(p, x, partner[e], y)
        return remote(dst, dst, zsend.at[e * 3 + p], zrecv.at[e * 3 + p], {"z": partner[e]})

    def d_copy(e, p):
        k = e * 3 + p
        if (e + p) % 2 == 0:
            block = place(p, x, partner[e], 1 - y)
            return remote(block, block, dsend.at[k], drecv.at[k], to_x)
        block = place(p, 1 - x, partner[e], y)
        return remote(block, block, dsend.at[k], drecv.at[k], to_y)

    def relay(e, p):
        (y_copy if (e + p) % 2 == 0 else x_copy)(e, p).wait_recv()
        d_copy(e, p).start()

    def turned(src, dst, p):
        def turn(j, carry):
            here = strip(j, 128)
            dst[p, here, :] = src[:, here].T.astype(jnp.bfloat16)
            return carry

        lax.fori_loop(0, src.shape[1] // 128, turn, 0)

    order = (2, 0, 1)
    for p, full in zip(order, (down_full, gate_full, up_full)):
        loads[(2, 3, 1)[p]].wait()
        if p == 2:
            wsend[p] = full[...].astype(jnp.bfloat16)
        else:
            turned(full, wsend, p)
        mine = wsend.at[p, strip(z, hidden_rows)]
        y_copy(0, p, mine).start()
        x_copy(0, p, mine).start()
        for e in (1, 3, 2):
            z_copy(e, p).start()
    for p in order:
        feed_w[p, x, :, strip(z * 2 + y, width)] = wsend[p, strip(z, hidden_rows)]

    def piece(state, s, h):
        return state["whole"].at[s, c, pl.ds(h * (rows // 2), rows // 2)]

    def spread(state, own):
        state["own"] = own
        for h in range(2):
            src = own.at[pl.ds(h * (rows // 2), rows // 2)]

            @pl.when(z < 3)
            def _():
                remote(src, piece(state, z, h), state["rs"].at[h], state["rr"].at[2 + h], {"z": z + 1}).start()

            @pl.when(z > 0)
            def _():
                remote(src, piece(state, z, h), state["ls"].at[h], state["lr"].at[2 + h], {"z": z - 1}).start()

        for h in range(2):
            src = own.at[pl.ds(h * (rows // 2), rows // 2)]
            remote(src, piece(state, z, h), state["cs"].at[z * 2 + h], state["cr"].at[z * 2 + h], to_c).start()
        state["whole"][z, c] = own[...]

    def beside(state, s, h):
        src = piece(state, s, h)
        return remote(src, src, state["cs"].at[s * 2 + h], state["cr"].at[s * 2 + h], to_c)

    def pass_on(state, k, h):
        slot = k * 2 + h

        @pl.when(z >= k)
        def _():
            s = lax.rem(z - k + 4, 4)
            src = piece(state, s, h)
            remote(src, src, state["rs"].at[slot], state["rr"].at[slot], to_c).wait_recv()

            @pl.when(z < 3)
            def _():
                remote(src, src, state["rs"].at[slot], state["rr"].at[slot + 2], {"z": z + 1}).start()

            beside(state, s, h).start()

        @pl.when(z + k < 4)
        def _():
            s = lax.rem(z + k, 4)
            src = piece(state, s, h)
            remote(src, src, state["ls"].at[slot], state["lr"].at[slot], to_c).wait_recv()

            @pl.when(z > 0)
            def _():
                remote(src, src, state["ls"].at[slot], state["lr"].at[slot + 2], {"z": z - 1}).start()

            beside(state, s, h).start()

    def spread_done(state):
        for k in range(4):
            for h in range(2):
                slot = k * 2 + h
                src = piece(state, z, h)

                @pl.when((z >= k) & (z < 3))
                def _():
                    remote(src, src, state["rs"].at[slot], state["rr"].at[slot], to_c).wait_send()

                @pl.when((z + k < 4) & (z > 0))
                def _():
                    remote(src, src, state["ls"].at[slot], state["lr"].at[slot], to_c).wait_send()

                beside(state, k, h).wait_send()

    for k, full in enumerate(mixer_full):
        loads[4 + k].wait()
        if k == 3:
            msend[k] = full[...].astype(jnp.bfloat16)
        else:
            turned(full, msend, k)
    for copy in trades:
        copy.wait_recv()
    spread(stages[0], own0)

    def m_place(px, pz, py):
        return mixer_w.at[:, px, :, strip(pz * 2 + py, width)]

    def m_y(e, src=None):
        dst = m_place(x, partner_of(e), y)
        return remote(dst if src is None else src, dst, mysend.at[e], myrecv.at[e], to_y)

    def m_x(e, src=None):
        dst = m_place(x, partner_of(e), y)
        return remote(dst if src is None else src, dst, mxsend.at[e], mxrecv.at[e], to_x)

    def m_z(e):
        src = msend.at[:, strip(partner_of(e), channel_rows)]
        return remote(src, m_place(x, z, y), mzsend.at[e], mzrecv.at[e], {"z": partner_of(e)})

    def m_d(e):
        if e % 2 == 0:
            block = m_place(x, partner[e], 1 - y)
            return remote(block, block, mdsend.at[e], mdrecv.at[e], to_x)
        block = m_place(1 - x, partner[e], y)
        return remote(block, block, mdsend.at[e], mdrecv.at[e], to_y)

    def m_relay(e):
        (m_y if e % 2 == 0 else m_x)(e).wait_recv()
        m_d(e).start()

    hops = [
        remote(part, part, ssend.at[slot], srecv.at[slot], target)
        for slot, (part, target) in zip(
            (0, 4, 5), ((blocks.at[c, x, y], to_y), (blocks.at[c, x], to_x), (blocks.at[c], to_c))
        )
    ]
    sent = [(0, p) for p in order]
    arriving = [(e, p) for p in order for e in (1, 3, 2)]
    for j, (e, p) in enumerate(arriving):
        z_landed(e, p).wait_recv()
        y_copy(e, p).start()
        x_copy(e, p).start()
        sent.append((e, p))
        relay(*sent[j])
        if j == 2:
            for copy in scale_sends:
                copy.wait_recv()
            hops[0].start()
        if j in (4, 6):
            hops[j // 2 - 2].wait_recv()
            hops[j // 2 - 1].start()
    for k in range(1, 4):
        for h in range(2):
            pass_on(stages[0], k, h)
    for e in (1, 3, 2):
        m_z(e).start()
    mine = msend.at[:, strip(z, channel_rows)]
    mixer_w[:, x, :, strip(z * 2 + y, width)] = msend[:, strip(z, channel_rows)]
    hops[2].wait_recv()

    wide = units.shape[1]
    unit_total = jnp.zeros(units.shape, jnp.float32)
    channel_total = jnp.zeros(channels.shape, jnp.float32)
    unit_part = scale_refs[0].shape[1]
    lane_part = scale_refs[2].shape[1]
    for px in range(2):
        for py in range(2):
            block = blocks[c, px, py, z]
            padded = jnp.concatenate([block, jnp.zeros((block.shape[0], wide - block.shape[1]), jnp.float32)], 1)
            k = px * 2 + py
            unit_total = unit_total + (pltpu.roll(padded, k * unit_part, 1) if k else padded)
            channel_total = channel_total + (pltpu.roll(block, k * lane_part, 1) if k else block)
    units[...] = unit_total
    channels[...] = channel_total
    pair = 2 * lane_part
    for px in range(2):
        for pc in range(CORES):
            for pz in range(4):
                low, high = (blocks[pc, px, py, pz][:, 0:pair] for py in range(2))
                start = ((px * CORES + pc) * 4 + pz) * pair
                lanes[:, start : start + pair] = low + pltpu.roll(high, lane_part, 1)
    for px in range(2):
        taps_own[:, px * pair : (px + 1) * pair] = taps_ref[:, strip((px * CORES + c) * 4 + z, pair)]

    for e, p in sent[len(arriving) :]:
        relay(e, p)
    m_y(0, mine).start()
    m_x(0, mine).start()
    for e, p in sent:
        (x_copy if (e + p) % 2 == 0 else y_copy)(e, p).wait_recv()
        d_copy(e, p).wait_recv()

    half_width = features // 2

    def to_near(state, e, h):
        return remote(
            state["sums"].at[e, h], state["got"].at[0, h], state["ps"].at[e * 2 + h], state["gr"].at[h], {"z": near}
        )

    def to_merge(state, e, h):
        slot = (5 - e) * 2 + h
        return remote(
            state["sums"].at[e, h], state["extra"].at[5 - e, h], state["ps"].at[e * 2 + h], state["er"].at[slot], {"z": near}
        )

    def to_far(state, e, h):
        return remote(
            state["sums"].at[e, h], state["got"].at[1, h], state["ps"].at[e * 2 + h], state["gr"].at[2 + h],
            {"z": partner[e]},
        )

    def handover(state, e, h):
        return remote(
            state["part"].at[e, h, 1 - c], state["half"].at[e, h], state["hs"].at[e * 2 + h], state["hr"].at[e * 2 + h], to_c
        )

    def run(number, units_of, weights, factors, before, pick):
        state = stages[number]
        exit_k = weights.shape[0] - 1

        def step(i, carry):
            before(i)
            e = pick(i)
            s = partner_of(e)
            for h in range(2):
                beside(state, s, h).wait_recv()
            inputs = state["whole"][s].reshape(CORES * rows, features)
            hidden = units_of(inputs, weights, factors, taps_own[...])
            for h in range(2):
                last = weights[exit_k, :, :, pl.ds(h * half_width, half_width)].reshape(-1, half_width)
                total = jnp.dot(hidden, last, preferred_element_type=jnp.float32)
                state["part"][e, h] = total.astype(jnp.bfloat16).reshape(CORES, rows, half_width)
                handover(state, e, h).start()
            for h in range(2):
                handover(state, e, h).wait_recv()
                both = state["part"][e, h, c].astype(jnp.float32) + state["half"][e, h].astype(jnp.float32)
                state["sums"][e, h] = both.astype(jnp.bfloat16)

                @pl.when(e == 1)
                def _():
                    to_near(state, 1, h).start()

                @pl.when((1 - middle) * e > 1)
                def _():
                    to_merge(state, e, h).start()

            return carry

        lax.fori_loop(0, 4, step, 0)

        @pl.when(middle == 1)
        def _():
            for e in (2, 3) if number == 0 else (3, 2):
                for h in range(2):
                    far = state["extra"].at[e, h]
                    remote(far, far, state["ps"].at[e * 2 + h], state["er"].at[e * 2 + h], to_c).wait_recv()
                    both = state["sums"][e, h].astype(jnp.float32) + state["extra"][e, h].astype(jnp.float32)
                    state["sums"][e, h] = both.astype(jnp.bfloat16)
                    to_far(state, e, h).start()

    def finish(number, out, factor):
        state = stages[number]
        own = state["own"]
        gain_ref, shift_ref = norms[number]
        scale_row = 6 if number == 1 else 5
        pieces, one, two = [], 0.0, 0.0
        for h in range(2):
            cols = slice(h * half_width, (h + 1) * half_width)
            total = state["sums"][0, h].astype(jnp.float32)
            for k in range(2):
                src = state["got"].at[k, h]
                remote(src, src, state["ps"].at[h], state["gr"].at[k * 2 + h], to_c).wait_recv()
                total = total + state["got"][k, h].astype(jnp.float32)
            scale = lanes[scale_row : scale_row + 1, cols] * factor
            summed = RESIDUAL_SCALE * own[:, cols].astype(jnp.float32) + total * scale
            pieces.append(summed)
            one = one + jnp.sum(summed, -1, keepdims=True)
            two = two + jnp.sum(summed * summed, -1, keepdims=True)
        average = one / features
        variance = two / features - average * average
        inverse = lax.rsqrt(variance + EPSILON)
        for h in range(2):
            cols = slice(h * half_width, (h + 1) * half_width)
            normed = (pieces[h] - average) * inverse * gain_ref[:, cols] + shift_ref[:, cols]
            out[:, cols] = normed.astype(jnp.bfloat16)

    def mixer_arrivals(i):
        @pl.when(i > 0)
        def _():
            e = later_third(i)
            landed = m_place(x, partner_of(e), y)
            remote(landed, landed, mzsend.at[e], mzrecv.at[e], to_c).wait_recv()
            m_y(e).start()
            m_x(e).start()

    def line_arrivals(state):
        def before(i):
            @pl.when(i == 1)
            def _():
                for h in range(2):
                    pass_on(state, 1, h)

            @pl.when(i == 2)
            def _():
                for h in range(2):
                    pass_on(state, 2, h)

            @pl.when(i == 3)
            def _():
                for h in range(2):
                    pass_on(state, 3, h)

        return before

    run(
        0, feed_units, feed_w, units[:, : 2 * hidden_rows], mixer_arrivals,
        lambda i: (1 - middle) * (3 - i) + middle * lax.rem(i + 1, 4),
    )
    m_relay(0)
    m_relay(1)
    finish(0, own1, HALF_STEP)
    spread(stages[1], own1)
    m_relay(3)
    m_relay(2)
    for e in range(4):
        (m_x if e % 2 == 0 else m_y)(e).wait_recv()
        m_d(e).wait_recv()

    def arrival_order(i):
        return (1 - middle) * i + middle * ((i + 2) // 3) * (lax.rem(i + 1, 3) + 1)

    run(1, mixer_units, mixer_w, channels[...], line_arrivals(stages[1]), arrival_order)
    finish(1, own2, 1.0)
    spread(stages[2], own2)
    run(2, feed_units, feed_w, units[:, : 2 * hidden_rows], line_arrivals(stages[2]), arrival_order)
    finish(2, sheet, HALF_STEP)

    here = strip(place_here, rows)
    leaving = []
    for k, (tx, tc) in enumerate(((1 - x, c), (1 - x, 1 - c), (x, 1 - c))):
        there = strip(tx * CORES + tc, columns)
        leaving.append(
            remote(sheet.at[:, there], out_ref.at[here], fsend.at[k], frecv.at[k], {"x": tx, "c": tc})
        )
        leaving[-1].start()
    out_ref[here] = sheet[:, strip(place_here, columns)]

    for copy in trades + scale_sends + hops:
        copy.wait_send()
    for e, p in sent:
        y_copy(e, p).wait_send()
        x_copy(e, p).wait_send()
        d_copy(e, p).wait_send()
        if e > 0:
            z_copy(e, p).wait_send()
    for e in range(4):
        m_y(e).wait_send()
        m_x(e).wait_send()
        m_d(e).wait_send()
        if e > 0:
            m_z(e).wait_send()
    for state in stages:
        spread_done(state)
        for e in range(4):
            for h in range(2):
                handover(state, e, h).wait_send()
                if e > 0:
                    to_near(state, e, h).wait_send()
    for copy in leaving:
        copy.wait()


def column_plan(
    depth, tokens, gate_weight, up_weight, down_weight, gate_scale, up_scale, down_scale,
    bgate_weight, cgate_weight, value_weight, bgate_scale, cgate_scale, value_scale, conv_taps,
    mixout_weight, mixout_scale, first_gain, first_shift, mixer_gain, mixer_shift, last_gain, last_shift,
):
    dma = pltpu.SemaphoreType.DMA
    low, full = jnp.bfloat16, jnp.float32
    rows = tokens.shape[0] // (2 * CORES)
    features = tokens.shape[1] * 2 * CORES
    half_width = features // 2
    width = gate_weight.shape[0]
    hidden = gate_weight.shape[1]
    channels = bgate_weight.shape[1]
    lanes = max(-(-gate_scale.shape[1] // 128) * 128, 4 * bgate_scale.shape[1])
    big = [gate_weight, up_weight, down_weight, bgate_weight, cgate_weight, value_weight, mixout_weight]
    scales = [gate_scale, up_scale, bgate_scale, cgate_scale, value_scale, down_scale, mixout_scale]
    vectors = [first_gain, first_shift, mixer_gain, mixer_shift, last_gain, last_shift]
    operands = [tokens, *big, *scales, conv_taps] + [v[None] for v in vectors]
    scratch = [pltpu.VMEM(tokens.shape, low)] + [pltpu.VMEM(w.shape, full) for w in big]
    scratch += [
        pltpu.VMEM((3, hidden, width), low),
        pltpu.VMEM((4, channels, width), low),
        pltpu.VMEM((3, 2, hidden // depth, features), low),
        pltpu.VMEM((4, 2, channels // depth, features), low),
        pltpu.VMEM((8, lanes), full),
        pltpu.VMEM((CORES, 2, 2, depth, 8, lanes), full),
        pltpu.VMEM((8, features), full),
        pltpu.VMEM((8, -(-2 * hidden // depth // 128) * 128), full),
        pltpu.VMEM((8, 2 * channels // depth), full),
        pltpu.VMEM((TAPS, 2 * channels // depth), full),
    ]
    scratch += [pltpu.VMEM((rows, features), low) for _ in range(4)]
    for _ in range(3):
        scratch += [
            pltpu.VMEM((depth, CORES, rows, features), low),
            pltpu.VMEM((depth, 2, CORES, rows, half_width), low),
            pltpu.VMEM((depth, 2, rows, half_width), low),
            pltpu.VMEM((depth, 2, rows, half_width), low),
            pltpu.VMEM((depth, 2, rows, half_width), low),
            pltpu.VMEM((2, 2, rows, half_width), low),
        ]
    scratch += [dma((8,)), dma((3,)), dma((3,)), dma((6,)), dma((6,)), dma((3,)), dma((3,))]
    scratch += [dma((12,)) for _ in range(8)]
    scratch += [dma((4,)) for _ in range(8)]
    for _ in range(3):
        scratch += [dma((10,)) for _ in range(4)] + [dma((8,)) for _ in range(7)]
    return pl.pallas_call(
        layer_kernel,
        out_shape=jax.ShapeDtypeStruct(tokens.shape, low),
        in_specs=[ANY] * 8 + [VMEM] * (len(operands) - 8),
        out_specs=VMEM,
        scratch_shapes=scratch,
        compiler_params=pltpu.CompilerParams(
            collective_id=0, has_side_effects=True, vmem_limit_bytes=60 * 1024 * 1024
        ),
        name="layer",
    )(*operands)


def add_rows(gathered, shard_piece):
    return jnp.dot(gathered, shard_piece, preferred_element_type=jnp.float32)


def features(inputs):
    return lax.all_gather(inputs, "tp", axis=1, tiled=True)


def post_norm(residual, branch, norm_gain, norm_shift):
    summed = RESIDUAL_SCALE * residual.astype(jnp.float32) + branch
    moments = lax.psum((jnp.sum(summed, -1), jnp.sum(summed * summed, -1)), "tp")
    feature_total = summed.shape[1] * lax.axis_size("tp")
    average = (moments[0] / feature_total)[:, None]
    mean_square = (moments[1] / feature_total)[:, None]
    variance = mean_square - average * average
    return ((summed - average) * lax.rsqrt(variance + EPSILON) * norm_gain + norm_shift).astype(
        jnp.bfloat16
    )


def spread_back(weight_cols, left_rows):
    return (
        lax.psum_scatter(
            lax.dot_general(
                weight_cols, left_rows, (((0,), (1,)), ((), ())), preferred_element_type=jnp.float32
            ).astype(jnp.bfloat16),
            "tp",
            scatter_dimension=0,
            tiled=True,
        )
        .astype(jnp.float32)
        .T
    )


def shards(
    tokens,
    gate_weight,
    up_weight,
    down_weight,
    gate_scale,
    up_scale,
    down_scale,
    bgate_weight,
    cgate_weight,
    value_weight,
    bgate_scale,
    cgate_scale,
    value_scale,
    conv_taps,
    mixout_weight,
    mixout_scale,
    first_gain,
    first_shift,
    mixer_gain,
    mixer_shift,
    last_gain,
    last_shift,
):
    scales = (
        lax.all_gather(gate_scale, "fs", axis=1, tiled=True),
        lax.all_gather(up_scale, "fs", axis=1, tiled=True),
        lax.all_gather(down_scale, "fs", axis=1, tiled=True),
        lax.all_gather(bgate_scale, "fs", axis=1, tiled=True),
        lax.all_gather(cgate_scale, "fs", axis=1, tiled=True),
        lax.all_gather(value_scale, "fs", axis=1, tiled=True),
        lax.all_gather(mixout_scale, "fs", axis=1, tiled=True),
    )
    gate_cols, up_cols, down_cols, bgate_cols, cgate_cols, value_cols, mixout_cols = [
        scale_row.reshape(-1) for scale_row in scales
    ]
    tp_index = lax.axis_index("tp")
    columns = tokens.shape[1]

    def own_part(vector):
        return lax.dynamic_slice_in_dim(vector, tp_index * columns, columns)

    gate_low = gate_weight.astype(jnp.bfloat16)
    up_low = up_weight.astype(jnp.bfloat16)
    down_low = down_weight.astype(jnp.bfloat16)
    kept_gate, kept_up = (
        lax.all_gather(gate_low, "fs", axis=0, tiled=True),
        lax.all_gather(up_low, "fs", axis=0, tiled=True),
    )
    kept_down = lax.all_gather(down_low, "fs", axis=1, tiled=True)

    def channel_mix(gathered):
        gate_sum = jnp.dot(gathered, kept_gate, preferred_element_type=jnp.float32)
        up_sum = jnp.dot(gathered, kept_up, preferred_element_type=jnp.float32)
        hidden = (jax.nn.silu(gate_sum * gate_cols) * (up_sum * up_cols)).astype(jnp.bfloat16)
        return HALF_STEP * (spread_back(kept_down, hidden) * down_cols)

    first = post_norm(
        tokens, channel_mix(features(tokens)), own_part(first_gain), own_part(first_shift)
    )
    gathered = features(first)
    bgate_low = bgate_weight.astype(jnp.bfloat16)
    channels = bgate_low.shape[1]
    outgate = add_rows(gathered, lax.all_gather(bgate_low, "fs", axis=0, tiled=True))
    ingate = add_rows(
        gathered, lax.all_gather(cgate_weight.astype(jnp.bfloat16), "fs", axis=0, tiled=True)
    )
    values = add_rows(
        gathered, lax.all_gather(value_weight.astype(jnp.bfloat16), "fs", axis=0, tiled=True)
    )
    tap_weights = lax.dynamic_slice_in_dim(conv_taps, tp_index * channels, channels, 1)
    mixed = (ingate * cgate_cols * (values * value_cols)).reshape(-1, LENGTH, channels)
    padded = jnp.pad(mixed, ((0, 0), (TAPS - 1, 0), (0, 0)))
    convolved = jnp.zeros(mixed.shape, jnp.float32)
    for tap_index in range(TAPS):
        convolved = convolved + tap_weights[tap_index] * padded[:, tap_index : tap_index + LENGTH]
    gated = (outgate * bgate_cols * convolved.reshape(-1, channels)).astype(jnp.bfloat16)
    mix_full = lax.all_gather(mixout_weight.astype(jnp.bfloat16), "fs", axis=1, tiled=True)
    second = post_norm(
        first,
        spread_back(mix_full, gated) * mixout_cols,
        own_part(mixer_gain),
        own_part(mixer_shift),
    )
    return post_norm(
        second, channel_mix(features(second)), own_part(last_gain), own_part(last_shift)
    )


def solution(mesh):
    in_specs = (
        P("fs", "tp"),
        P("fs", "tp"),
        P("fs", "tp"),
        P("tp", "fs"),
        P("tp", "fs"),
        P("tp", "fs"),
        P("tp", "fs"),
        P("fs", "tp"),
        P("fs", "tp"),
        P("fs", "tp"),
        P("tp", "fs"),
        P("tp", "fs"),
        P("tp", "fs"),
        P(),
        P("tp", "fs"),
        P("tp", "fs"),
        P(),
        P(),
        P(),
        P(),
        P(),
        P(),
    )
    out_specs = P("fs", "tp")
    across = mesh.shape["tp"] // CORES
    if across == 2 and mesh.shape["fs"] == 8:
        depth = mesh.shape["fs"] // 2
        fine = Mesh(mesh.devices.reshape(depth, 2, 2, CORES), ("z", "y", "x", "c"))
        names = {"fs": ("z", "y"), "tp": ("x", "c")}

        def split(spec):
            return P(*(names.get(name) for name in spec))

        return jax.shard_map(
            functools.partial(column_plan, depth),
            mesh=fine,
            in_specs=tuple(split(spec) for spec in in_specs),
            out_specs=split(out_specs),
            check_vma=False,
        )
    return jax.shard_map(shards, mesh=mesh, in_specs=in_specs, out_specs=out_specs, check_vma=False)
```

```python
import functools

import jax
import jax.numpy as jnp
from jax import lax
from jax.experimental import pallas as pl
from jax.experimental.pallas import tpu as pltpu
from jax.sharding import Mesh
from jax.sharding import PartitionSpec as P

TAPS = 3
LENGTH = 128
CORES = 2
ROW_CUTS = 2
COLUMN_CUTS = 2

RESIDUAL_SCALE = 1.4142135623730951
HALF_STEP = 0.5
EPSILON = 1e-05
BY_AXIS = pl.DeviceIdType.MESH
HBM = pl.BlockSpec(memory_space=pltpu.HBM)
VMEM = pl.BlockSpec(memory_space=pltpu.VMEM)


def remote(src, dst, send, recv, target):
    return pltpu.make_async_remote_copy(
        src_ref=src, dst_ref=dst, send_sem=send, recv_sem=recv, device_id=target, device_id_type=BY_AXIS
    )


def dot_last(left, right):
    return lax.dot_general(left, right, (((1,), (1,)), ((), ())), preferred_element_type=jnp.float32)


def merged(ref, k):
    two, rows, features = ref.shape[1:]
    return ref[k].reshape(two * rows, features)


def feed_units(inputs, weights, factors, taps):
    gate_sum = dot_last(inputs, merged(weights, 0)) * factors[0:1]
    up_sum = dot_last(inputs, merged(weights, 1)) * factors[1:2]
    return (gate_sum / (1.0 + jnp.exp(-gate_sum)) * up_sum).astype(jnp.bfloat16)


def mixer_units(inputs, weights, factors, taps):
    outgate = dot_last(inputs, merged(weights, 0)) * factors[2:3]
    ingate = dot_last(inputs, merged(weights, 1)) * factors[3:4]
    values = dot_last(inputs, merged(weights, 2)) * factors[4:5]
    mixed = ingate * values
    position = lax.rem(lax.broadcasted_iota(jnp.int32, mixed.shape, 0), LENGTH)
    convolved = taps[TAPS - 1 : TAPS] * mixed
    for back in range(1, TAPS):
        earlier = jnp.where(position >= back, pltpu.roll(mixed, back, 0), 0.0)
        convolved = convolved + taps[TAPS - 1 - back : TAPS - back] * earlier
    return (outgate * convolved).astype(jnp.bfloat16)


def later_third(i):
    return i + (i // 2) * (5 - 2 * i)


def layer_kernel(
    tokens_ref, gate_ref, up_ref, down_ref, b_ref, c_ref, v_ref, mix_ref, *refs
):
    refs = list(refs)
    take = lambda n: [refs.pop(0) for _ in range(n)]
    small = take(14)
    (out_ref,) = take(1)
    held = take(14)
    scale_refs, taps_ref = held[:7], held[7]
    norms = [held[8 + 2 * k : 10 + 2 * k] for k in range(3)]
    tin, gate_full, up_full, down_full, *mixer_full = take(8)
    wsend, msend, feed_w, mixer_w, pack, blocks, lanes, units, channels, taps_own = take(10)
    own0, own1, own2, sheet = take(4)
    stages = [dict(zip(("whole", "part", "half", "sums", "extra", "got"), take(6))) for _ in range(3)]
    local, asend, arecv, ssend, srecv, fsend, frecv = take(7)
    zsend, zrecv, ysend, yrecv, xsend, xrecv, dsend, drecv = take(8)
    mzsend, mzrecv, mysend, myrecv, mxsend, mxrecv, mdsend, mdrecv = take(8)
    for state in stages:
        names = ("rs", "rr", "ls", "lr", "cs", "cr", "hs", "hr", "ps", "gr", "er")
        state.update(zip(names, take(len(names))))

    z, y, x, c = (lax.axis_index(axis) for axis in ("z", "y", "x", "c"))
    near = z + 1 - 2 * lax.rem(z, 2)
    cross = lax.rem(z + 2, 4)
    opposite = 3 - z
    middle = lax.rem((z + 1) // 2, 2)
    partner = (z, near, cross, opposite)
    to_x, to_y, to_c = {"x": 1 - x}, {"y": 1 - y}, {"c": 1 - c}

    def partner_of(e):
        odd = 1 - 2 * lax.rem(z, 2)
        return lax.rem(z + odd * lax.rem(e, 2) + 2 * (e // 2), 4)

    loads = [
        pltpu.make_async_copy(src, dst, local.at[k])
        for k, (src, dst) in enumerate(
            zip(
                (tokens_ref, down_ref, gate_ref, up_ref, b_ref, c_ref, v_ref, mix_ref),
                (tin, down_full, gate_full, up_full, *mixer_full),
            )
        )
    ]
    little = [pltpu.make_async_copy(src, dst, local.at[8 + k]) for k, (src, dst) in enumerate(zip(small, held))]
    for load in little[:7] + loads + little[7:]:
        load.start()
    barrier = pltpu.get_barrier_semaphore()
    greeted = [{"z": t} for t in partner[1:]] + [to_x, to_y, to_c, {"x": 1 - x, "c": 1 - c}]
    for target in greeted:
        pl.semaphore_signal(barrier, inc=1, device_id=target, device_id_type=BY_AXIS)
    pack[...] = jnp.zeros_like(pack)
    for k, scale_ref in enumerate(scale_refs):
        little[k].wait()
        pack[k : k + 1, 0 : scale_ref.shape[1]] = scale_ref[...]
    pl.semaphore_wait(barrier, len(greeted))

    scale_sends = []
    for e in (1, 2, 3):
        scale_sends.append(remote(pack, blocks.at[c, x, y, z], ssend.at[e], srecv.at[e], {"z": partner[e]}))
        scale_sends[-1].start()
    blocks[c, x, y, z] = pack[...]

    rows, features = own0.shape
    columns = tin.shape[1]
    place_here = x * CORES + c

    def strip(t, width):
        return pl.ds(pl.multiple_of(t * width, width), width)

    loads[0].wait()
    trades = []
    for k, (tx, tc) in enumerate(((1 - x, c), (1 - x, 1 - c), (x, 1 - c))):
        trades.append(
            remote(
                tin.at[strip(tx * CORES + tc, rows)],
                own0.at[:, strip(place_here, columns)],
                asend.at[k],
                arecv.at[k],
                {"x": tx, "c": tc},
            )
        )
        trades[-1].start()
    own0[:, strip(place_here, columns)] = tin[strip(place_here, rows)]

    hidden_rows, width = feed_w.shape[2], wsend.shape[2]
    channel_rows = mixer_w.shape[2]

    def place(p, px, pz, py):
        return feed_w.at[p, px, :, strip(pz * 2 + py, width)]

    def y_copy(e, p, src=None):
        dst = place(p, x, partner[e], y)
        return remote(dst if src is None else src, dst, ysend.at[e * 3 + p], yrecv.at[e * 3 + p], to_y)

    def x_copy(e, p, src=None):
        dst = place(p, x, partner[e], y)
        return remote(dst if src is None else src, dst, xsend.at[e * 3 + p], xrecv.at[e * 3 + p], to_x)

    def z_copy(e, p):
        src = wsend.at[p, strip(partner[e], hidden_rows)]
        return remote(src, place(p, x, z, y), zsend.at[e * 3 + p], zrecv.at[e * 3 + p], {"z": partner[e]})

    def z_landed(e, p):
        dst = place(p, x, partner[e], y)
        return remote(dst, dst, zsend.at[e * 3 + p], zrecv.at[e * 3 + p], {"z": partner[e]})

    def d_copy(e, p):
        k = e * 3 + p
        if (e + p) % 2 == 0:
            block = place(p, x, partner[e], 1 - y)
            return remote(block, block, dsend.at[k], drecv.at[k], to_x)
        block = place(p, 1 - x, partner[e], y)
        return remote(block, block, dsend.at[k], drecv.at[k], to_y)

    def relay(e, p):
        (y_copy if (e + p) % 2 == 0 else x_copy)(e, p).wait_recv()
        d_copy(e, p).start()

    def turned(src, dst, p):
        def turn(j, carry):
            here = strip(j, 128)
            dst[p, here, :] = src[:, here].T.astype(jnp.bfloat16)
            return carry

        lax.fori_loop(0, src.shape[1] // 128, turn, 0)

    order = (2, 0, 1)
    for p, full in zip(order, (down_full, gate_full, up_full)):
        loads[(2, 3, 1)[p]].wait()
        if p == 2:
            wsend[p] = full[...].astype(jnp.bfloat16)
        else:
            turned(full, wsend, p)
        mine = wsend.at[p, strip(z, hidden_rows)]
        y_copy(0, p, mine).start()
        x_copy(0, p, mine).start()
        for e in (1, 3, 2):
            z_copy(e, p).start()
    for p in order:
        feed_w[p, x, :, strip(z * 2 + y, width)] = wsend[p, strip(z, hidden_rows)]

    cut_rows = rows // ROW_CUTS

    def piece(state, s, h):
        return state["whole"].at[s, c, pl.ds(h * cut_rows, cut_rows)]

    def beside(state, s, h, src=None):
        dst = piece(state, s, h)
        slot = s * ROW_CUTS + h
        return remote(dst if src is None else src, dst, state["cs"].at[slot], state["cr"].at[slot], to_c)

    def rightward(state, s, k, h, src=None):
        dst = piece(state, s, h)
        slot = k * ROW_CUTS + h
        return remote(
            dst if src is None else src, dst, state["rs"].at[slot], state["rr"].at[slot + ROW_CUTS], {"z": z + 1}
        )

    def leftward(state, s, k, h, src=None):
        dst = piece(state, s, h)
        slot = k * ROW_CUTS + h
        return remote(
            dst if src is None else src, dst, state["ls"].at[slot], state["lr"].at[slot + ROW_CUTS], {"z": z - 1}
        )

    def spread(state, own):
        state["own"] = own
        for h in range(ROW_CUTS):
            src = own.at[pl.ds(h * cut_rows, cut_rows)]

            @pl.when(z < 3)
            def _():
                rightward(state, z, 0, h, src).start()

            @pl.when(z > 0)
            def _():
                leftward(state, z, 0, h, src).start()

            beside(state, z, h, src).start()
        state["whole"][z, c] = own[...]

    def pass_on(state, k, h):
        slot = k * ROW_CUTS + h

        @pl.when(z >= k)
        def _():
            s = lax.rem(z - k + 4, 4)
            src = piece(state, s, h)
            remote(src, src, state["rs"].at[slot], state["rr"].at[slot], to_c).wait_recv()

            @pl.when(z < 3)
            def _():
                rightward(state, s, k, h).start()

            beside(state, s, h).start()

        @pl.when(z + k < 4)
        def _():
            s = lax.rem(z + k, 4)
            src = piece(state, s, h)
            remote(src, src, state["ls"].at[slot], state["lr"].at[slot], to_c).wait_recv()

            @pl.when(z > 0)
            def _():
                leftward(state, s, k, h).start()

            beside(state, s, h).start()

    def spread_done(state):
        for k in range(4):
            for h in range(ROW_CUTS):

                @pl.when((z >= k) & (z < 3))
                def _():
                    rightward(state, z, k, h).wait_send()

                @pl.when((z + k < 4) & (z > 0))
                def _():
                    leftward(state, z, k, h).wait_send()

                beside(state, k, h).wait_send()

    for k, full in enumerate(mixer_full):
        loads[4 + k].wait()
        if k == 3:
            msend[k] = full[...].astype(jnp.bfloat16)
        else:
            turned(full, msend, k)
    for copy in trades:
        copy.wait_recv()
    spread(stages[0], own0)

    def m_place(px, pz, py):
        return mixer_w.at[:, px, :, strip(pz * 2 + py, width)]

    def m_y(e, src=None):
        dst = m_place(x, partner_of(e), y)
        return remote(dst if src is None else src, dst, mysend.at[e], myrecv.at[e], to_y)

    def m_x(e, src=None):
        dst = m_place(x, partner_of(e), y)
        return remote(dst if src is None else src, dst, mxsend.at[e], mxrecv.at[e], to_x)

    def m_z(e):
        src = msend.at[:, strip(partner_of(e), channel_rows)]
        return remote(src, m_place(x, z, y), mzsend.at[e], mzrecv.at[e], {"z": partner_of(e)})

    def m_d(e):
        mats = mixer_w.shape[0] // 2
        over_y = m_place(x, partner[e], 1 - y).at[pl.ds(0, mats)]
        over_x = m_place(1 - x, partner[e], y).at[pl.ds(mats, mats)]
        return (
            remote(over_y, over_y, mdsend.at[2 * e], mdrecv.at[2 * e], to_x),
            remote(over_x, over_x, mdsend.at[2 * e + 1], mdrecv.at[2 * e + 1], to_y),
        )

    def m_relay(e):
        for arrival, copy in zip((m_y, m_x), m_d(e)):
            arrival(e).wait_recv()
            copy.start()

    hops = [
        remote(part, part, ssend.at[slot], srecv.at[slot], target)
        for slot, (part, target) in zip(
            (0, 4, 5), ((blocks.at[c, x, y], to_y), (blocks.at[c, x], to_x), (blocks.at[c], to_c))
        )
    ]
    sent = [(0, p) for p in order]
    arriving = [(e, p) for p in order for e in (1, 3, 2)]
    for j, (e, p) in enumerate(arriving):
        z_landed(e, p).wait_recv()
        y_copy(e, p).start()
        x_copy(e, p).start()
        sent.append((e, p))
        relay(*sent[j])
        if j == 2:
            for copy in scale_sends:
                copy.wait_recv()
            hops[0].start()
        if j in (4, 6):
            hops[j // 2 - 2].wait_recv()
            hops[j // 2 - 1].start()
    for k in range(1, 4):
        for h in range(ROW_CUTS):
            pass_on(stages[0], k, h)
    for e in (1, 3, 2):
        m_z(e).start()
    mine = msend.at[:, strip(z, channel_rows)]
    mixer_w[:, x, :, strip(z * 2 + y, width)] = msend[:, strip(z, channel_rows)]
    hops[2].wait_recv()

    wide = units.shape[1]
    unit_total = jnp.zeros(units.shape, jnp.float32)
    channel_total = jnp.zeros(channels.shape, jnp.float32)
    unit_part = scale_refs[0].shape[1]
    lane_part = scale_refs[2].shape[1]
    for px in range(2):
        for py in range(2):
            block = blocks[c, px, py, z]
            padded = jnp.concatenate([block, jnp.zeros((block.shape[0], wide - block.shape[1]), jnp.float32)], 1)
            k = px * 2 + py
            unit_total = unit_total + (pltpu.roll(padded, k * unit_part, 1) if k else padded)
            channel_total = channel_total + (pltpu.roll(block, k * lane_part, 1) if k else block)
    units[...] = unit_total
    channels[...] = channel_total
    pair = 2 * lane_part
    for px in range(2):
        for pc in range(CORES):
            for pz in range(4):
                low, high = (blocks[pc, px, py, pz][:, 0:pair] for py in range(2))
                start = ((px * CORES + pc) * 4 + pz) * pair
                lanes[:, start : start + pair] = low + pltpu.roll(high, lane_part, 1)
    for load in little[7:]:
        load.wait()
    for px in range(2):
        taps_own[:, px * pair : (px + 1) * pair] = taps_ref[:, strip((px * CORES + c) * 4 + z, pair)]

    for e, p in sent[len(arriving) :]:
        relay(e, p)
    m_y(0, mine).start()
    m_x(0, mine).start()
    for e, p in sent:
        (x_copy if (e + p) % 2 == 0 else y_copy)(e, p).wait_recv()
        d_copy(e, p).wait_recv()

    cut_width = features // COLUMN_CUTS
    cuts = range(COLUMN_CUTS)

    def to_near(state, e, h):
        return remote(
            state["sums"].at[e, h], state["got"].at[0, h], state["ps"].at[e * COLUMN_CUTS + h], state["gr"].at[h],
            {"z": near},
        )

    def to_merge(state, e, h):
        slot = (5 - e) * COLUMN_CUTS + h
        return remote(
            state["sums"].at[e, h], state["extra"].at[5 - e, h], state["ps"].at[e * COLUMN_CUTS + h],
            state["er"].at[slot], {"z": near},
        )

    def to_far(state, e, h):
        return remote(
            state["sums"].at[e, h], state["got"].at[1, h], state["ps"].at[e * COLUMN_CUTS + h],
            state["gr"].at[COLUMN_CUTS + h], {"z": partner[e]},
        )

    def handover(state, e, h):
        slot = e * COLUMN_CUTS + h
        return remote(
            state["part"].at[e, h, 1 - c], state["half"].at[e, h], state["hs"].at[slot], state["hr"].at[slot], to_c
        )

    def run(number, units_of, weights, factors, before, pick):
        state = stages[number]
        exit_k = weights.shape[0] - 1

        def step(i, carry):
            before(i)
            e = pick(i)
            s = partner_of(e)
            for h in range(ROW_CUTS):
                beside(state, s, h).wait_recv()
            inputs = state["whole"][s].reshape(CORES * rows, features)
            hidden = units_of(inputs, weights, factors, taps_own[...])
            for h in cuts:
                last = weights[exit_k, :, :, pl.ds(h * cut_width, cut_width)].reshape(-1, cut_width)
                total = jnp.dot(hidden, last, preferred_element_type=jnp.float32)
                state["part"][e, h] = total.astype(jnp.bfloat16).reshape(CORES, rows, cut_width)
                handover(state, e, h).start()
            for h in cuts:
                handover(state, e, h).wait_recv()
                both = state["part"][e, h, c].astype(jnp.float32) + state["half"][e, h].astype(jnp.float32)
                state["sums"][e, h] = both.astype(jnp.bfloat16)

                @pl.when(e == 1)
                def _():
                    to_near(state, 1, h).start()

                @pl.when((1 - middle) * e > 1)
                def _():
                    to_merge(state, e, h).start()

            return carry

        lax.fori_loop(0, 4, step, 0)

        @pl.when(middle == 1)
        def _():
            for e in (2, 3) if number == 0 else (3, 2):
                for h in cuts:
                    far = state["extra"].at[e, h]
                    remote(far, far, state["ps"].at[h], state["er"].at[e * COLUMN_CUTS + h], to_c).wait_recv()
                    both = state["sums"][e, h].astype(jnp.float32) + state["extra"][e, h].astype(jnp.float32)
                    state["sums"][e, h] = both.astype(jnp.bfloat16)
                    to_far(state, e, h).start()

    def finish(number, out, factor):
        state = stages[number]
        own = state["own"]
        gain_ref, shift_ref = norms[number]
        scale_row = 6 if number == 1 else 5
        pieces, one, two = [], 0.0, 0.0
        for h in cuts:
            cols = slice(h * cut_width, (h + 1) * cut_width)
            total = state["sums"][0, h].astype(jnp.float32)
            for k in range(2):
                src = state["got"].at[k, h]
                remote(src, src, state["ps"].at[h], state["gr"].at[k * COLUMN_CUTS + h], to_c).wait_recv()
                total = total + state["got"][k, h].astype(jnp.float32)
            scale = lanes[scale_row : scale_row + 1, cols] * factor
            summed = RESIDUAL_SCALE * own[:, cols].astype(jnp.float32) + total * scale
            pieces.append(summed)
            one = one + jnp.sum(summed, -1, keepdims=True)
            two = two + jnp.sum(summed * summed, -1, keepdims=True)
        average = one / features
        variance = two / features - average * average
        inverse = lax.rsqrt(variance + EPSILON)
        for h in cuts:
            cols = slice(h * cut_width, (h + 1) * cut_width)
            normed = (pieces[h] - average) * inverse * gain_ref[:, cols] + shift_ref[:, cols]
            out[:, cols] = normed.astype(jnp.bfloat16)

    def mixer_arrivals(i):
        @pl.when(i > 0)
        def _():
            e = later_third(i)
            landed = m_place(x, partner_of(e), y)
            remote(landed, landed, mzsend.at[e], mzrecv.at[e], to_c).wait_recv()
            m_y(e).start()
            m_x(e).start()

    def arrival_order(i):
        return (1 - middle) * i + middle * ((i + 2) // 3) * (lax.rem(i + 1, 3) + 1)

    def pass_all(state, k):
        for h in range(ROW_CUTS):
            pass_on(state, k, h)

    def arrivals_second(i):
        pl.when((i == 1) & (middle == 0))(lambda: pass_all(stages[1], 2))
        pl.when(i == 2)(lambda: pass_all(stages[1], 3))

    def arrivals_third(i):
        pl.when(i == 1)(lambda: pass_all(stages[2], 1))
        pl.when(i == 2 - middle)(lambda: pass_all(stages[2], 2))
        pl.when(i == 3)(lambda: pass_all(stages[2], 3))

    run(
        0, feed_units, feed_w, units[:, : 2 * hidden_rows], mixer_arrivals,
        lambda i: (1 - middle) * (3 - i) + middle * lax.rem(i + 1, 4),
    )
    m_relay(0)
    m_relay(1)
    m_relay(3)
    finish(0, own1, HALF_STEP)
    spread(stages[1], own1)
    pl.when(middle == 1)(lambda: pass_all(stages[1], 1))
    m_relay(2)
    pl.when(middle == 0)(lambda: pass_all(stages[1], 1))
    pl.when(middle == 1)(lambda: pass_all(stages[1], 2))
    for e in range(4):
        for copy in m_d(e):
            copy.wait_recv()
    run(
        1, mixer_units, mixer_w, channels[...], arrivals_second,
        lambda i: arrival_order(lax.rem(i + 1, 4)),
    )
    finish(1, own2, 1.0)
    spread(stages[2], own2)
    run(2, feed_units, feed_w, units[:, : 2 * hidden_rows], arrivals_third, arrival_order)
    finish(2, sheet, HALF_STEP)

    here = strip(place_here, rows)
    leaving = []
    for k, (tx, tc) in enumerate(((1 - x, c), (1 - x, 1 - c), (x, 1 - c))):
        there = strip(tx * CORES + tc, columns)
        leaving.append(
            remote(sheet.at[:, there], out_ref.at[here], fsend.at[k], frecv.at[k], {"x": tx, "c": tc})
        )
        leaving[-1].start()
    out_ref[here] = sheet[:, strip(place_here, columns)]

    for copy in trades + scale_sends + hops:
        copy.wait_send()
    for e, p in sent:
        y_copy(e, p).wait_send()
        x_copy(e, p).wait_send()
        d_copy(e, p).wait_send()
        if e > 0:
            z_copy(e, p).wait_send()
    for e in range(4):
        m_y(e).wait_send()
        m_x(e).wait_send()
        for copy in m_d(e):
            copy.wait_send()
        if e > 0:
            m_z(e).wait_send()
    for state in stages:
        spread_done(state)
        for e in range(4):
            for h in cuts:
                handover(state, e, h).wait_send()
                if e > 0:
                    to_near(state, e, h).wait_send()
    for copy in leaving:
        copy.wait()


def column_plan(
    depth, tokens, gate_weight, up_weight, down_weight, gate_scale, up_scale, down_scale,
    bgate_weight, cgate_weight, value_weight, bgate_scale, cgate_scale, value_scale, conv_taps,
    mixout_weight, mixout_scale, first_gain, first_shift, mixer_gain, mixer_shift, last_gain, last_shift,
):
    dma = pltpu.SemaphoreType.DMA
    low, full = jnp.bfloat16, jnp.float32
    rows = tokens.shape[0] // (2 * CORES)
    features = tokens.shape[1] * 2 * CORES
    cut_width = features // COLUMN_CUTS
    width = gate_weight.shape[0]
    hidden = gate_weight.shape[1]
    channels = bgate_weight.shape[1]
    lanes = max(-(-gate_scale.shape[1] // 128) * 128, 4 * bgate_scale.shape[1])
    big = [gate_weight, up_weight, down_weight, bgate_weight, cgate_weight, value_weight, mixout_weight]
    scales = [gate_scale, up_scale, bgate_scale, cgate_scale, value_scale, down_scale, mixout_scale]
    vectors = [first_gain, first_shift, mixer_gain, mixer_shift, last_gain, last_shift]
    operands = [tokens, *big, *scales, conv_taps] + [v[None] for v in vectors]
    scratch = [pltpu.VMEM(operand.shape, full) for operand in operands[8:]]
    scratch += [pltpu.VMEM(tokens.shape, low)] + [pltpu.VMEM(w.shape, full) for w in big]
    scratch += [
        pltpu.VMEM((3, hidden, width), low),
        pltpu.VMEM((4, channels, width), low),
        pltpu.VMEM((3, 2, hidden // depth, features), low),
        pltpu.VMEM((4, 2, channels // depth, features), low),
        pltpu.VMEM((8, lanes), full),
        pltpu.VMEM((CORES, 2, 2, depth, 8, lanes), full),
        pltpu.VMEM((8, features), full),
        pltpu.VMEM((8, -(-2 * hidden // depth // 128) * 128), full),
        pltpu.VMEM((8, 2 * channels // depth), full),
        pltpu.VMEM((TAPS, 2 * channels // depth), full),
    ]
    scratch += [pltpu.VMEM((rows, features), low) for _ in range(4)]
    for _ in range(3):
        scratch += [
            pltpu.VMEM((depth, CORES, rows, features), low),
            pltpu.VMEM((depth, COLUMN_CUTS, CORES, rows, cut_width), low),
            pltpu.VMEM((depth, COLUMN_CUTS, rows, cut_width), low),
            pltpu.VMEM((depth, COLUMN_CUTS, rows, cut_width), low),
            pltpu.VMEM((depth, COLUMN_CUTS, rows, cut_width), low),
            pltpu.VMEM((2, COLUMN_CUTS, rows, cut_width), low),
        ]
    scratch += [dma((len(operands),)), dma((3,)), dma((3,)), dma((6,)), dma((6,)), dma((3,)), dma((3,))]
    scratch += [dma((12,)) for _ in range(8)]
    scratch += [dma((4,)) for _ in range(6)] + [dma((8,)) for _ in range(2)]
    for _ in range(3):
        scratch += [dma((5 * ROW_CUTS,)) for _ in range(6)] + [dma((4 * COLUMN_CUTS,)) for _ in range(5)]
    return pl.pallas_call(
        layer_kernel,
        out_shape=jax.ShapeDtypeStruct(tokens.shape, low),
        in_specs=[HBM] * len(operands),
        out_specs=VMEM,
        scratch_shapes=scratch,
        compiler_params=pltpu.CompilerParams(
            collective_id=0, has_side_effects=True, vmem_limit_bytes=60 * 1024 * 1024
        ),
        name="layer",
    )(*operands)


def add_rows(gathered, shard_piece):
    return jnp.dot(gathered, shard_piece, preferred_element_type=jnp.float32)


def features(inputs):
    return lax.all_gather(inputs, "tp", axis=1, tiled=True)


def post_norm(residual, branch, norm_gain, norm_shift):
    summed = RESIDUAL_SCALE * residual.astype(jnp.float32) + branch
    moments = lax.psum((jnp.sum(summed, -1), jnp.sum(summed * summed, -1)), "tp")
    feature_total = summed.shape[1] * lax.axis_size("tp")
    average = (moments[0] / feature_total)[:, None]
    mean_square = (moments[1] / feature_total)[:, None]
    variance = mean_square - average * average
    return ((summed - average) * lax.rsqrt(variance + EPSILON) * norm_gain + norm_shift).astype(
        jnp.bfloat16
    )


def spread_back(weight_cols, left_rows):
    return (
        lax.psum_scatter(
            lax.dot_general(
                weight_cols, left_rows, (((0,), (1,)), ((), ())), preferred_element_type=jnp.float32
            ).astype(jnp.bfloat16),
            "tp",
            scatter_dimension=0,
            tiled=True,
        )
        .astype(jnp.float32)
        .T
    )


def shards(
    tokens,
    gate_weight,
    up_weight,
    down_weight,
    gate_scale,
    up_scale,
    down_scale,
    bgate_weight,
    cgate_weight,
    value_weight,
    bgate_scale,
    cgate_scale,
    value_scale,
    conv_taps,
    mixout_weight,
    mixout_scale,
    first_gain,
    first_shift,
    mixer_gain,
    mixer_shift,
    last_gain,
    last_shift,
):
    scales = (
        lax.all_gather(gate_scale, "fs", axis=1, tiled=True),
        lax.all_gather(up_scale, "fs", axis=1, tiled=True),
        lax.all_gather(down_scale, "fs", axis=1, tiled=True),
        lax.all_gather(bgate_scale, "fs", axis=1, tiled=True),
        lax.all_gather(cgate_scale, "fs", axis=1, tiled=True),
        lax.all_gather(value_scale, "fs", axis=1, tiled=True),
        lax.all_gather(mixout_scale, "fs", axis=1, tiled=True),
    )
    gate_cols, up_cols, down_cols, bgate_cols, cgate_cols, value_cols, mixout_cols = [
        scale_row.reshape(-1) for scale_row in scales
    ]
    tp_index = lax.axis_index("tp")
    columns = tokens.shape[1]

    def own_part(vector):
        return lax.dynamic_slice_in_dim(vector, tp_index * columns, columns)

    gate_low = gate_weight.astype(jnp.bfloat16)
    up_low = up_weight.astype(jnp.bfloat16)
    down_low = down_weight.astype(jnp.bfloat16)
    kept_gate, kept_up = (
        lax.all_gather(gate_low, "fs", axis=0, tiled=True),
        lax.all_gather(up_low, "fs", axis=0, tiled=True),
    )
    kept_down = lax.all_gather(down_low, "fs", axis=1, tiled=True)

    def channel_mix(gathered):
        gate_sum = jnp.dot(gathered, kept_gate, preferred_element_type=jnp.float32)
        up_sum = jnp.dot(gathered, kept_up, preferred_element_type=jnp.float32)
        hidden = (jax.nn.silu(gate_sum * gate_cols) * (up_sum * up_cols)).astype(jnp.bfloat16)
        return HALF_STEP * (spread_back(kept_down, hidden) * down_cols)

    first = post_norm(
        tokens, channel_mix(features(tokens)), own_part(first_gain), own_part(first_shift)
    )
    gathered = features(first)
    bgate_low = bgate_weight.astype(jnp.bfloat16)
    channels = bgate_low.shape[1]
    outgate = add_rows(gathered, lax.all_gather(bgate_low, "fs", axis=0, tiled=True))
    ingate = add_rows(
        gathered, lax.all_gather(cgate_weight.astype(jnp.bfloat16), "fs", axis=0, tiled=True)
    )
    values = add_rows(
        gathered, lax.all_gather(value_weight.astype(jnp.bfloat16), "fs", axis=0, tiled=True)
    )
    tap_weights = lax.dynamic_slice_in_dim(conv_taps, tp_index * channels, channels, 1)
    mixed = (ingate * cgate_cols * (values * value_cols)).reshape(-1, LENGTH, channels)
    padded = jnp.pad(mixed, ((0, 0), (TAPS - 1, 0), (0, 0)))
    convolved = jnp.zeros(mixed.shape, jnp.float32)
    for tap_index in range(TAPS):
        convolved = convolved + tap_weights[tap_index] * padded[:, tap_index : tap_index + LENGTH]
    gated = (outgate * bgate_cols * convolved.reshape(-1, channels)).astype(jnp.bfloat16)
    mix_full = lax.all_gather(mixout_weight.astype(jnp.bfloat16), "fs", axis=1, tiled=True)
    second = post_norm(
        first,
        spread_back(mix_full, gated) * mixout_cols,
        own_part(mixer_gain),
        own_part(mixer_shift),
    )
    return post_norm(
        second, channel_mix(features(second)), own_part(last_gain), own_part(last_shift)
    )


def solution(mesh):
    in_specs = (
        P("fs", "tp"),
        P("fs", "tp"),
        P("fs", "tp"),
        P("tp", "fs"),
        P("tp", "fs"),
        P("tp", "fs"),
        P("tp", "fs"),
        P("fs", "tp"),
        P("fs", "tp"),
        P("fs", "tp"),
        P("tp", "fs"),
        P("tp", "fs"),
        P("tp", "fs"),
        P(),
        P("tp", "fs"),
        P("tp", "fs"),
        P(),
        P(),
        P(),
        P(),
        P(),
        P(),
    )
    out_specs = P("fs", "tp")
    across = mesh.shape["tp"] // CORES
    if across == 2 and mesh.shape["fs"] == 8:
        depth = mesh.shape["fs"] // 2
        fine = Mesh(mesh.devices.reshape(depth, 2, 2, CORES), ("z", "y", "x", "c"))
        names = {"fs": ("z", "y"), "tp": ("x", "c")}

        def split(spec):
            return P(*(names.get(name) for name in spec))

        return jax.shard_map(
            functools.partial(column_plan, depth),
            mesh=fine,
            in_specs=tuple(split(spec) for spec in in_specs),
            out_specs=split(out_specs),
            check_vma=False,
        )
    return jax.shard_map(shards, mesh=mesh, in_specs=in_specs, out_specs=out_specs, check_vma=False)
```

```python
import functools

import jax
import jax.numpy as jnp
from jax import lax
from jax.experimental import pallas as pl
from jax.experimental.pallas import tpu as pltpu
from jax.sharding import Mesh
from jax.sharding import PartitionSpec as P

TAPS = 3
LENGTH = 128
CORES = 2
ROW_CUTS = 2
COLUMN_CUTS = 2

RESIDUAL_SCALE = 1.4142135623730951
HALF_STEP = 0.5
EPSILON = 1e-05
BY_AXIS = pl.DeviceIdType.MESH
HBM = pl.BlockSpec(memory_space=pltpu.HBM)
VMEM = pl.BlockSpec(memory_space=pltpu.VMEM)


def remote(src, dst, send, recv, target):
    return pltpu.make_async_remote_copy(
        src_ref=src, dst_ref=dst, send_sem=send, recv_sem=recv, device_id=target, device_id_type=BY_AXIS
    )


def dot_last(left, right):
    return lax.dot_general(left, right, (((1,), (1,)), ((), ())), preferred_element_type=jnp.float32)


def merged(ref, k):
    two, rows, features = ref.shape[1:]
    return ref[k].reshape(two * rows, features)


def feed_units(inputs, weights, factors, taps):
    gate_sum = dot_last(inputs, merged(weights, 0)) * factors[0:1]
    up_sum = dot_last(inputs, merged(weights, 1)) * factors[1:2]
    return (gate_sum / (1.0 + jnp.exp(-gate_sum)) * up_sum).astype(jnp.bfloat16)


def mixer_units(inputs, weights, factors, taps):
    outgate = dot_last(inputs, merged(weights, 0)) * factors[2:3]
    ingate = dot_last(inputs, merged(weights, 1)) * factors[3:4]
    values = dot_last(inputs, merged(weights, 2)) * factors[4:5]
    mixed = ingate * values
    position = lax.rem(lax.broadcasted_iota(jnp.int32, mixed.shape, 0), LENGTH)
    convolved = taps[TAPS - 1 : TAPS] * mixed
    for back in range(1, TAPS):
        earlier = jnp.where(position >= back, pltpu.roll(mixed, back, 0), 0.0)
        convolved = convolved + taps[TAPS - 1 - back : TAPS - back] * earlier
    return (outgate * convolved).astype(jnp.bfloat16)


def later_third(i):
    return i + (i // 2) * (5 - 2 * i)


def layer_kernel(
    tokens_ref, gate_ref, up_ref, down_ref, b_ref, c_ref, v_ref, mix_ref, *refs
):
    refs = list(refs)
    take = lambda n: [refs.pop(0) for _ in range(n)]
    small = take(14)
    (out_ref,) = take(1)
    held = take(14)
    scale_refs, taps_ref = held[:7], held[7]
    norms = [held[8 + 2 * k : 10 + 2 * k] for k in range(3)]
    tin, gate_full, up_full, down_full, *mixer_full = take(8)
    wsend, msend, feed_w, mixer_w, pack, blocks, lanes, units, channels, taps_own = take(10)
    own0, own1, own2, sheet = take(4)
    stages = [dict(zip(("whole", "part", "half", "sums", "extra", "got"), take(6))) for _ in range(3)]
    local, asend, arecv, ssend, srecv, fsend, frecv = take(7)
    zsend, zrecv, ysend, yrecv, xsend, xrecv, dsend, drecv = take(8)
    mzsend, mzrecv, mysend, myrecv, mxsend, mxrecv, mdsend, mdrecv = take(8)
    for state in stages:
        names = ("rs", "rr", "ls", "lr", "cs", "cr", "hs", "hr", "ps", "gr", "er")
        state.update(zip(names, take(len(names))))

    z, y, x, c = (lax.axis_index(axis) for axis in ("z", "y", "x", "c"))
    near = z + 1 - 2 * lax.rem(z, 2)
    cross = lax.rem(z + 2, 4)
    opposite = 3 - z
    middle = lax.rem((z + 1) // 2, 2)
    partner = (z, near, cross, opposite)
    to_x, to_y, to_c = {"x": 1 - x}, {"y": 1 - y}, {"c": 1 - c}

    def partner_of(e):
        odd = 1 - 2 * lax.rem(z, 2)
        return lax.rem(z + odd * lax.rem(e, 2) + 2 * (e // 2), 4)

    loads = [
        pltpu.make_async_copy(src, dst, local.at[k])
        for k, (src, dst) in enumerate(
            zip(
                (tokens_ref, down_ref, gate_ref, up_ref, b_ref, c_ref, v_ref, mix_ref),
                (tin, down_full, gate_full, up_full, *mixer_full),
            )
        )
    ]
    little = [pltpu.make_async_copy(src, dst, local.at[8 + k]) for k, (src, dst) in enumerate(zip(small, held))]
    for load in little[:7] + loads + little[7:]:
        load.start()
    barrier = pltpu.get_barrier_semaphore()
    greeted = [{"z": t} for t in partner[1:]] + [to_x, to_y, to_c, {"x": 1 - x, "c": 1 - c}]
    for target in greeted:
        pl.semaphore_signal(barrier, inc=1, device_id=target, device_id_type=BY_AXIS)
    pack[...] = jnp.zeros_like(pack)
    for k, scale_ref in enumerate(scale_refs):
        little[k].wait()
        pack[k : k + 1, 0 : scale_ref.shape[1]] = scale_ref[...]
    pl.semaphore_wait(barrier, len(greeted))

    scale_sends = []
    for e in (1, 2, 3):
        scale_sends.append(remote(pack, blocks.at[c, x, y, z], ssend.at[e], srecv.at[e], {"z": partner[e]}))
        scale_sends[-1].start()
    blocks[c, x, y, z] = pack[...]

    rows, features = own0.shape
    columns = tin.shape[1]
    place_here = x * CORES + c

    def strip(t, width):
        return pl.ds(pl.multiple_of(t * width, width), width)

    loads[0].wait()
    trades = []
    for k, (tx, tc) in enumerate(((1 - x, c), (1 - x, 1 - c), (x, 1 - c))):
        trades.append(
            remote(
                tin.at[strip(tx * CORES + tc, rows)],
                own0.at[:, strip(place_here, columns)],
                asend.at[k],
                arecv.at[k],
                {"x": tx, "c": tc},
            )
        )
        trades[-1].start()
    own0[:, strip(place_here, columns)] = tin[strip(place_here, rows)]

    hidden_rows, width = feed_w.shape[2], wsend.shape[2]
    channel_rows = mixer_w.shape[2]

    def place(p, px, pz, py):
        return feed_w.at[p, px, :, strip(pz * 2 + py, width)]

    def y_copy(e, p, src=None):
        dst = place(p, x, partner[e], y)
        return remote(dst if src is None else src, dst, ysend.at[e * 3 + p], yrecv.at[e * 3 + p], to_y)

    def x_copy(e, p, src=None):
        dst = place(p, x, partner[e], y)
        return remote(dst if src is None else src, dst, xsend.at[e * 3 + p], xrecv.at[e * 3 + p], to_x)

    def z_copy(e, p):
        src = wsend.at[p, strip(partner[e], hidden_rows)]
        return remote(src, place(p, x, z, y), zsend.at[e * 3 + p], zrecv.at[e * 3 + p], {"z": partner[e]})

    def z_landed(e, p):
        dst = place(p, x, partner[e], y)
        return remote(dst, dst, zsend.at[e * 3 + p], zrecv.at[e * 3 + p], {"z": partner[e]})

    def d_copy(e, p):
        k = e * 3 + p
        if (e + p) % 2 == 0:
            block = place(p, x, partner[e], 1 - y)
            return remote(block, block, dsend.at[k], drecv.at[k], to_x)
        block = place(p, 1 - x, partner[e], y)
        return remote(block, block, dsend.at[k], drecv.at[k], to_y)

    def relay(e, p):
        (y_copy if (e + p) % 2 == 0 else x_copy)(e, p).wait_recv()
        d_copy(e, p).start()

    def turned(src, dst, p):
        def turn(j, carry):
            here = strip(j, 128)
            dst[p, here, :] = src[:, here].T.astype(jnp.bfloat16)
            return carry

        lax.fori_loop(0, src.shape[1] // 128, turn, 0)

    order = (2, 0, 1)
    for p, full in zip(order, (down_full, gate_full, up_full)):
        loads[(2, 3, 1)[p]].wait()
        if p == 2:
            wsend[p] = full[...].astype(jnp.bfloat16)
        else:
            turned(full, wsend, p)
        mine = wsend.at[p, strip(z, hidden_rows)]
        y_copy(0, p, mine).start()
        x_copy(0, p, mine).start()
        for e in (1, 3, 2):
            z_copy(e, p).start()
    for p in order:
        feed_w[p, x, :, strip(z * 2 + y, width)] = wsend[p, strip(z, hidden_rows)]

    cut_rows = rows // ROW_CUTS

    def piece(state, s, h):
        return state["whole"].at[s, c, pl.ds(h * cut_rows, cut_rows)]

    def beside(state, s, h, src=None):
        dst = piece(state, s, h)
        slot = s * ROW_CUTS + h
        return remote(dst if src is None else src, dst, state["cs"].at[slot], state["cr"].at[slot], to_c)

    def rightward(state, s, k, h, src=None):
        dst = piece(state, s, h)
        slot = k * ROW_CUTS + h
        return remote(
            dst if src is None else src, dst, state["rs"].at[slot], state["rr"].at[slot + ROW_CUTS], {"z": z + 1}
        )

    def leftward(state, s, k, h, src=None):
        dst = piece(state, s, h)
        slot = k * ROW_CUTS + h
        return remote(
            dst if src is None else src, dst, state["ls"].at[slot], state["lr"].at[slot + ROW_CUTS], {"z": z - 1}
        )

    def spread(state, own):
        state["own"] = own
        for h in range(ROW_CUTS):
            src = own.at[pl.ds(h * cut_rows, cut_rows)]

            @pl.when(z < 3)
            def _():
                rightward(state, z, 0, h, src).start()

            @pl.when(z > 0)
            def _():
                leftward(state, z, 0, h, src).start()

            beside(state, z, h, src).start()
        state["whole"][z, c] = own[...]

    def pass_right(state, k, h):
        slot = k * ROW_CUTS + h

        @pl.when(z >= k)
        def _():
            s = lax.rem(z - k + 4, 4)
            src = piece(state, s, h)
            remote(src, src, state["rs"].at[slot], state["rr"].at[slot], to_c).wait_recv()

            @pl.when(z < 3)
            def _():
                rightward(state, s, k, h).start()

            beside(state, s, h).start()

    def pass_left(state, k, h):
        slot = k * ROW_CUTS + h

        @pl.when(z + k < 4)
        def _():
            s = lax.rem(z + k, 4)
            src = piece(state, s, h)
            remote(src, src, state["ls"].at[slot], state["lr"].at[slot], to_c).wait_recv()

            @pl.when(z > 0)
            def _():
                leftward(state, s, k, h).start()

            beside(state, s, h).start()

    def sooner(state, k):
        for h in range(ROW_CUTS):
            pl.when(z < 2)(lambda: pass_left(state, k, h))
            pl.when(z >= 2)(lambda: pass_right(state, k, h))

    def later(state, k):
        for h in range(ROW_CUTS):
            pl.when(z < 2)(lambda: pass_right(state, k, h))
            pl.when(z >= 2)(lambda: pass_left(state, k, h))

    def pass_all(state, k):
        sooner(state, k)
        later(state, k)

    def spread_done(state):
        for k in range(4):
            for h in range(ROW_CUTS):

                @pl.when((z >= k) & (z < 3))
                def _():
                    rightward(state, z, k, h).wait_send()

                @pl.when((z + k < 4) & (z > 0))
                def _():
                    leftward(state, z, k, h).wait_send()

                beside(state, k, h).wait_send()

    for k, full in enumerate(mixer_full):
        loads[4 + k].wait()
        if k == 3:
            msend[k] = full[...].astype(jnp.bfloat16)
        else:
            turned(full, msend, k)
    for copy in trades:
        copy.wait_recv()
    spread(stages[0], own0)

    def m_place(px, pz, py):
        return mixer_w.at[:, px, :, strip(pz * 2 + py, width)]

    def m_y(e, src=None):
        dst = m_place(x, partner_of(e), y)
        return remote(dst if src is None else src, dst, mysend.at[e], myrecv.at[e], to_y)

    def m_x(e, src=None):
        dst = m_place(x, partner_of(e), y)
        return remote(dst if src is None else src, dst, mxsend.at[e], mxrecv.at[e], to_x)

    def m_z(e):
        src = msend.at[:, strip(partner_of(e), channel_rows)]
        return remote(src, m_place(x, z, y), mzsend.at[e], mzrecv.at[e], {"z": partner_of(e)})

    def m_d(e):
        mats = mixer_w.shape[0] // 2
        over_y = m_place(x, partner[e], 1 - y).at[pl.ds(0, mats)]
        over_x = m_place(1 - x, partner[e], y).at[pl.ds(mats, mats)]
        return (
            remote(over_y, over_y, mdsend.at[2 * e], mdrecv.at[2 * e], to_x),
            remote(over_x, over_x, mdsend.at[2 * e + 1], mdrecv.at[2 * e + 1], to_y),
        )

    def m_relay(e):
        for arrival, copy in zip((m_y, m_x), m_d(e)):
            arrival(e).wait_recv()
            copy.start()

    hops = [
        remote(part, part, ssend.at[slot], srecv.at[slot], target)
        for slot, (part, target) in zip(
            (0, 4, 5), ((blocks.at[c, x, y], to_y), (blocks.at[c, x], to_x), (blocks.at[c], to_c))
        )
    ]
    sent = [(0, p) for p in order]
    arriving = [(e, p) for p in order for e in (1, 3, 2)]
    for j, (e, p) in enumerate(arriving):
        z_landed(e, p).wait_recv()
        y_copy(e, p).start()
        x_copy(e, p).start()
        sent.append((e, p))
        relay(*sent[j])
        if j == 2:
            for copy in scale_sends:
                copy.wait_recv()
            hops[0].start()
        if j in (4, 6):
            hops[j // 2 - 2].wait_recv()
            hops[j // 2 - 1].start()
    for k in range(1, 4):
        for h in range(ROW_CUTS):
            pass_right(stages[0], k, h)
            pass_left(stages[0], k, h)
    for e in (1, 3, 2):
        m_z(e).start()
    mine = msend.at[:, strip(z, channel_rows)]
    mixer_w[:, x, :, strip(z * 2 + y, width)] = msend[:, strip(z, channel_rows)]
    hops[2].wait_recv()

    wide = units.shape[1]
    unit_total = jnp.zeros(units.shape, jnp.float32)
    channel_total = jnp.zeros(channels.shape, jnp.float32)
    unit_part = scale_refs[0].shape[1]
    lane_part = scale_refs[2].shape[1]
    for px in range(2):
        for py in range(2):
            block = blocks[c, px, py, z]
            padded = jnp.concatenate([block, jnp.zeros((block.shape[0], wide - block.shape[1]), jnp.float32)], 1)
            k = px * 2 + py
            unit_total = unit_total + (pltpu.roll(padded, k * unit_part, 1) if k else padded)
            channel_total = channel_total + (pltpu.roll(block, k * lane_part, 1) if k else block)
    units[...] = unit_total
    channels[...] = channel_total
    pair = 2 * lane_part
    for px in range(2):
        for pc in range(CORES):
            for pz in range(4):
                low, high = (blocks[pc, px, py, pz][:, 0:pair] for py in range(2))
                start = ((px * CORES + pc) * 4 + pz) * pair
                lanes[:, start : start + pair] = low + pltpu.roll(high, lane_part, 1)
    for load in little[7:]:
        load.wait()
    for px in range(2):
        taps_own[:, px * pair : (px + 1) * pair] = taps_ref[:, strip((px * CORES + c) * 4 + z, pair)]

    for e, p in sent[len(arriving) :]:
        relay(e, p)
    m_y(0, mine).start()
    m_x(0, mine).start()
    for e, p in sent:
        (x_copy if (e + p) % 2 == 0 else y_copy)(e, p).wait_recv()
        d_copy(e, p).wait_recv()

    cut_width = features // COLUMN_CUTS
    cuts = range(COLUMN_CUTS)

    def to_near(state, e, h):
        return remote(
            state["sums"].at[e, h], state["got"].at[0, h], state["ps"].at[e * COLUMN_CUTS + h], state["gr"].at[h],
            {"z": near},
        )

    def to_merge(state, e, h):
        slot = (5 - e) * COLUMN_CUTS + h
        return remote(
            state["sums"].at[e, h], state["extra"].at[5 - e, h], state["ps"].at[e * COLUMN_CUTS + h],
            state["er"].at[slot], {"z": near},
        )

    def to_far(state, e, h):
        return remote(
            state["sums"].at[e, h], state["got"].at[1, h], state["ps"].at[e * COLUMN_CUTS + h],
            state["gr"].at[COLUMN_CUTS + h], {"z": partner[e]},
        )

    def handover(state, e, h):
        slot = e * COLUMN_CUTS + h
        return remote(
            state["part"].at[e, h, 1 - c], state["half"].at[e, h], state["hs"].at[slot], state["hr"].at[slot], to_c
        )

    def run(number, units_of, weights, factors, before, pick):
        state = stages[number]
        exit_k = weights.shape[0] - 1

        def step(i, carry):
            before(i)
            e = pick(i)
            s = partner_of(e)
            for h in range(ROW_CUTS):
                beside(state, s, h).wait_recv()
            inputs = state["whole"][s].reshape(CORES * rows, features)
            hidden = units_of(inputs, weights, factors, taps_own[...])
            for h in cuts:
                last = weights[exit_k, :, :, pl.ds(h * cut_width, cut_width)].reshape(-1, cut_width)
                total = jnp.dot(hidden, last, preferred_element_type=jnp.float32)
                state["part"][e, h] = total.astype(jnp.bfloat16).reshape(CORES, rows, cut_width)
                handover(state, e, h).start()
            for h in cuts:
                handover(state, e, h).wait_recv()
                both = state["part"][e, h, c].astype(jnp.float32) + state["half"][e, h].astype(jnp.float32)
                state["sums"][e, h] = both.astype(jnp.bfloat16)

                @pl.when(e == 1)
                def _():
                    to_near(state, 1, h).start()

                @pl.when((1 - middle) * e > 1)
                def _():
                    to_merge(state, e, h).start()

            return carry

        lax.fori_loop(0, 4, step, 0)

        @pl.when(middle == 1)
        def _():
            for e in (2, 3) if number == 0 else (3, 2):
                for h in cuts:
                    far = state["extra"].at[e, h]
                    remote(far, far, state["ps"].at[h], state["er"].at[e * COLUMN_CUTS + h], to_c).wait_recv()
                    both = state["sums"][e, h].astype(jnp.float32) + state["extra"][e, h].astype(jnp.float32)
                    state["sums"][e, h] = both.astype(jnp.bfloat16)
                    to_far(state, e, h).start()

    def finish(number, out, factor):
        state = stages[number]
        own = state["own"]
        gain_ref, shift_ref = norms[number]
        scale_row = 6 if number == 1 else 5
        pieces, one, two = [], 0.0, 0.0
        for h in cuts:
            cols = slice(h * cut_width, (h + 1) * cut_width)
            total = state["sums"][0, h].astype(jnp.float32)
            for k in range(2):
                src = state["got"].at[k, h]
                remote(src, src, state["ps"].at[h], state["gr"].at[k * COLUMN_CUTS + h], to_c).wait_recv()
                total = total + state["got"][k, h].astype(jnp.float32)
            scale = lanes[scale_row : scale_row + 1, cols] * factor
            summed = RESIDUAL_SCALE * own[:, cols].astype(jnp.float32) + total * scale
            pieces.append(summed)
            one = one + jnp.sum(summed, -1, keepdims=True)
            two = two + jnp.sum(summed * summed, -1, keepdims=True)
        average = one / features
        variance = two / features - average * average
        inverse = lax.rsqrt(variance + EPSILON)
        for h in cuts:
            cols = slice(h * cut_width, (h + 1) * cut_width)
            normed = (pieces[h] - average) * inverse * gain_ref[:, cols] + shift_ref[:, cols]
            out[:, cols] = normed.astype(jnp.bfloat16)

    def mixer_arrivals(i):
        @pl.when(i > 0)
        def _():
            e = later_third(i)
            landed = m_place(x, partner_of(e), y)
            remote(landed, landed, mzsend.at[e], mzrecv.at[e], to_c).wait_recv()
            m_y(e).start()
            m_x(e).start()

    def arrival_order(i):
        return (1 - middle) * i + middle * ((i + 2) // 3) * (lax.rem(i + 1, 3) + 1)

    def arrivals_second(i):
        pl.when((i == 1) & (middle == 0))(lambda: pass_all(stages[1], 2))
        pl.when(i == 2)(lambda: pass_all(stages[1], 3))

    def arrivals_third(i):
        pl.when(i == 1)(lambda: pass_all(stages[2], 1))
        pl.when(i == 2 - middle)(lambda: pass_all(stages[2], 2))
        pl.when(i == 3)(lambda: pass_all(stages[2], 3))

    run(
        0, feed_units, feed_w, units[:, : 2 * hidden_rows], mixer_arrivals,
        lambda i: (1 - middle) * (3 - i) + middle * lax.rem(i + 1, 4),
    )
    m_relay(0)
    m_relay(1)
    m_relay(3)
    finish(0, own1, HALF_STEP)
    spread(stages[1], own1)
    pl.when(middle == 1)(lambda: pass_all(stages[1], 1))
    m_relay(2)
    pl.when(middle == 0)(lambda: pass_all(stages[1], 1))
    pl.when(middle == 1)(lambda: pass_all(stages[1], 2))
    for e in range(4):
        for copy in m_d(e):
            copy.wait_recv()
    run(
        1, mixer_units, mixer_w, channels[...], arrivals_second,
        lambda i: arrival_order(lax.rem(i + 1, 4)),
    )
    finish(1, own2, 1.0)
    spread(stages[2], own2)
    run(2, feed_units, feed_w, units[:, : 2 * hidden_rows], arrivals_third, arrival_order)
    finish(2, sheet, HALF_STEP)

    here = strip(place_here, rows)
    leaving = []
    for k, (tx, tc) in enumerate(((1 - x, c), (1 - x, 1 - c), (x, 1 - c))):
        there = strip(tx * CORES + tc, columns)
        leaving.append(
            remote(sheet.at[:, there], out_ref.at[here], fsend.at[k], frecv.at[k], {"x": tx, "c": tc})
        )
        leaving[-1].start()
    out_ref[here] = sheet[:, strip(place_here, columns)]

    for copy in trades + scale_sends + hops:
        copy.wait_send()
    for e, p in sent:
        y_copy(e, p).wait_send()
        x_copy(e, p).wait_send()
        d_copy(e, p).wait_send()
        if e > 0:
            z_copy(e, p).wait_send()
    for e in range(4):
        m_y(e).wait_send()
        m_x(e).wait_send()
        for copy in m_d(e):
            copy.wait_send()
        if e > 0:
            m_z(e).wait_send()
    for state in stages:
        spread_done(state)
        for e in range(4):
            for h in cuts:
                handover(state, e, h).wait_send()
                if e > 0:
                    to_near(state, e, h).wait_send()
    for copy in leaving:
        copy.wait()


def column_plan(
    depth, tokens, gate_weight, up_weight, down_weight, gate_scale, up_scale, down_scale,
    bgate_weight, cgate_weight, value_weight, bgate_scale, cgate_scale, value_scale, conv_taps,
    mixout_weight, mixout_scale, first_gain, first_shift, mixer_gain, mixer_shift, last_gain, last_shift,
):
    dma = pltpu.SemaphoreType.DMA
    low, full = jnp.bfloat16, jnp.float32
    rows = tokens.shape[0] // (2 * CORES)
    features = tokens.shape[1] * 2 * CORES
    cut_width = features // COLUMN_CUTS
    width = gate_weight.shape[0]
    hidden = gate_weight.shape[1]
    channels = bgate_weight.shape[1]
    lanes = max(-(-gate_scale.shape[1] // 128) * 128, 4 * bgate_scale.shape[1])
    big = [gate_weight, up_weight, down_weight, bgate_weight, cgate_weight, value_weight, mixout_weight]
    scales = [gate_scale, up_scale, bgate_scale, cgate_scale, value_scale, down_scale, mixout_scale]
    vectors = [first_gain, first_shift, mixer_gain, mixer_shift, last_gain, last_shift]
    operands = [tokens, *big, *scales, conv_taps] + [v[None] for v in vectors]
    scratch = [pltpu.VMEM(operand.shape, full) for operand in operands[8:]]
    scratch += [pltpu.VMEM(tokens.shape, low)] + [pltpu.VMEM(w.shape, full) for w in big]
    scratch += [
        pltpu.VMEM((3, hidden, width), low),
        pltpu.VMEM((4, channels, width), low),
        pltpu.VMEM((3, 2, hidden // depth, features), low),
        pltpu.VMEM((4, 2, channels // depth, features), low),
        pltpu.VMEM((8, lanes), full),
        pltpu.VMEM((CORES, 2, 2, depth, 8, lanes), full),
        pltpu.VMEM((8, features), full),
        pltpu.VMEM((8, -(-2 * hidden // depth // 128) * 128), full),
        pltpu.VMEM((8, 2 * channels // depth), full),
        pltpu.VMEM((TAPS, 2 * channels // depth), full),
    ]
    scratch += [pltpu.VMEM((rows, features), low) for _ in range(4)]
    for _ in range(3):
        scratch += [
            pltpu.VMEM((depth, CORES, rows, features), low),
            pltpu.VMEM((depth, COLUMN_CUTS, CORES, rows, cut_width), low),
            pltpu.VMEM((depth, COLUMN_CUTS, rows, cut_width), low),
            pltpu.VMEM((depth, COLUMN_CUTS, rows, cut_width), low),
            pltpu.VMEM((depth, COLUMN_CUTS, rows, cut_width), low),
            pltpu.VMEM((2, COLUMN_CUTS, rows, cut_width), low),
        ]
    scratch += [dma((len(operands),)), dma((3,)), dma((3,)), dma((6,)), dma((6,)), dma((3,)), dma((3,))]
    scratch += [dma((12,)) for _ in range(8)]
    scratch += [dma((4,)) for _ in range(6)] + [dma((8,)) for _ in range(2)]
    for _ in range(3):
        scratch += [dma((5 * ROW_CUTS,)) for _ in range(6)] + [dma((4 * COLUMN_CUTS,)) for _ in range(5)]
    return pl.pallas_call(
        layer_kernel,
        out_shape=jax.ShapeDtypeStruct(tokens.shape, low),
        in_specs=[HBM] * len(operands),
        out_specs=VMEM,
        scratch_shapes=scratch,
        compiler_params=pltpu.CompilerParams(
            collective_id=0, has_side_effects=True, vmem_limit_bytes=60 * 1024 * 1024
        ),
        name="layer",
    )(*operands)


def add_rows(gathered, shard_piece):
    return jnp.dot(gathered, shard_piece, preferred_element_type=jnp.float32)


def features(inputs):
    return lax.all_gather(inputs, "tp", axis=1, tiled=True)


def post_norm(residual, branch, norm_gain, norm_shift):
    summed = RESIDUAL_SCALE * residual.astype(jnp.float32) + branch
    moments = lax.psum((jnp.sum(summed, -1), jnp.sum(summed * summed, -1)), "tp")
    feature_total = summed.shape[1] * lax.axis_size("tp")
    average = (moments[0] / feature_total)[:, None]
    mean_square = (moments[1] / feature_total)[:, None]
    variance = mean_square - average * average
    return ((summed - average) * lax.rsqrt(variance + EPSILON) * norm_gain + norm_shift).astype(
        jnp.bfloat16
    )


def spread_back(weight_cols, left_rows):
    return (
        lax.psum_scatter(
            lax.dot_general(
                weight_cols, left_rows, (((0,), (1,)), ((), ())), preferred_element_type=jnp.float32
            ).astype(jnp.bfloat16),
            "tp",
            scatter_dimension=0,
            tiled=True,
        )
        .astype(jnp.float32)
        .T
    )


def shards(
    tokens,
    gate_weight,
    up_weight,
    down_weight,
    gate_scale,
    up_scale,
    down_scale,
    bgate_weight,
    cgate_weight,
    value_weight,
    bgate_scale,
    cgate_scale,
    value_scale,
    conv_taps,
    mixout_weight,
    mixout_scale,
    first_gain,
    first_shift,
    mixer_gain,
    mixer_shift,
    last_gain,
    last_shift,
):
    scales = (
        lax.all_gather(gate_scale, "fs", axis=1, tiled=True),
        lax.all_gather(up_scale, "fs", axis=1, tiled=True),
        lax.all_gather(down_scale, "fs", axis=1, tiled=True),
        lax.all_gather(bgate_scale, "fs", axis=1, tiled=True),
        lax.all_gather(cgate_scale, "fs", axis=1, tiled=True),
        lax.all_gather(value_scale, "fs", axis=1, tiled=True),
        lax.all_gather(mixout_scale, "fs", axis=1, tiled=True),
    )
    gate_cols, up_cols, down_cols, bgate_cols, cgate_cols, value_cols, mixout_cols = [
        scale_row.reshape(-1) for scale_row in scales
    ]
    tp_index = lax.axis_index("tp")
    columns = tokens.shape[1]

    def own_part(vector):
        return lax.dynamic_slice_in_dim(vector, tp_index * columns, columns)

    gate_low = gate_weight.astype(jnp.bfloat16)
    up_low = up_weight.astype(jnp.bfloat16)
    down_low = down_weight.astype(jnp.bfloat16)
    kept_gate, kept_up = (
        lax.all_gather(gate_low, "fs", axis=0, tiled=True),
        lax.all_gather(up_low, "fs", axis=0, tiled=True),
    )
    kept_down = lax.all_gather(down_low, "fs", axis=1, tiled=True)

    def channel_mix(gathered):
        gate_sum = jnp.dot(gathered, kept_gate, preferred_element_type=jnp.float32)
        up_sum = jnp.dot(gathered, kept_up, preferred_element_type=jnp.float32)
        hidden = (jax.nn.silu(gate_sum * gate_cols) * (up_sum * up_cols)).astype(jnp.bfloat16)
        return HALF_STEP * (spread_back(kept_down, hidden) * down_cols)

    first = post_norm(
        tokens, channel_mix(features(tokens)), own_part(first_gain), own_part(first_shift)
    )
    gathered = features(first)
    bgate_low = bgate_weight.astype(jnp.bfloat16)
    channels = bgate_low.shape[1]
    outgate = add_rows(gathered, lax.all_gather(bgate_low, "fs", axis=0, tiled=True))
    ingate = add_rows(
        gathered, lax.all_gather(cgate_weight.astype(jnp.bfloat16), "fs", axis=0, tiled=True)
    )
    values = add_rows(
        gathered, lax.all_gather(value_weight.astype(jnp.bfloat16), "fs", axis=0, tiled=True)
    )
    tap_weights = lax.dynamic_slice_in_dim(conv_taps, tp_index * channels, channels, 1)
    mixed = (ingate * cgate_cols * (values * value_cols)).reshape(-1, LENGTH, channels)
    padded = jnp.pad(mixed, ((0, 0), (TAPS - 1, 0), (0, 0)))
    convolved = jnp.zeros(mixed.shape, jnp.float32)
    for tap_index in range(TAPS):
        convolved = convolved + tap_weights[tap_index] * padded[:, tap_index : tap_index + LENGTH]
    gated = (outgate * bgate_cols * convolved.reshape(-1, channels)).astype(jnp.bfloat16)
    mix_full = lax.all_gather(mixout_weight.astype(jnp.bfloat16), "fs", axis=1, tiled=True)
    second = post_norm(
        first,
        spread_back(mix_full, gated) * mixout_cols,
        own_part(mixer_gain),
        own_part(mixer_shift),
    )
    return post_norm(
        second, channel_mix(features(second)), own_part(last_gain), own_part(last_shift)
    )


def solution(mesh):
    in_specs = (
        P("fs", "tp"),
        P("fs", "tp"),
        P("fs", "tp"),
        P("tp", "fs"),
        P("tp", "fs"),
        P("tp", "fs"),
        P("tp", "fs"),
        P("fs", "tp"),
        P("fs", "tp"),
        P("fs", "tp"),
        P("tp", "fs"),
        P("tp", "fs"),
        P("tp", "fs"),
        P(),
        P("tp", "fs"),
        P("tp", "fs"),
        P(),
        P(),
        P(),
        P(),
        P(),
        P(),
    )
    out_specs = P("fs", "tp")
    across = mesh.shape["tp"] // CORES
    if across == 2 and mesh.shape["fs"] == 8:
        depth = mesh.shape["fs"] // 2
        fine = Mesh(mesh.devices.reshape(depth, 2, 2, CORES), ("z", "y", "x", "c"))
        names = {"fs": ("z", "y"), "tp": ("x", "c")}

        def split(spec):
            return P(*(names.get(name) for name in spec))

        return jax.shard_map(
            functools.partial(column_plan, depth),
            mesh=fine,
            in_specs=tuple(split(spec) for spec in in_specs),
            out_specs=split(out_specs),
            check_vma=False,
        )
    return jax.shard_map(shards, mesh=mesh, in_specs=in_specs, out_specs=out_specs, check_vma=False)
```
